128 devices in a mesh: sp: 64 (over z, y, x), tp: 2 (over core).
Axes of the slice: x: 4, y: 4, z: 4, core: 2. Of those that a mesh axis runs over, the one named last changes fastest.
Arguments:
- gate_pre: bfloat16 [16384, 2048], P('sp', 'tp'), may hold values from -6 to 6
- conv_in: bfloat16 [16384, 2048], P('sp', 'tp'), may hold values from -6 to 6
- conv_taps: bfloat16 [4, 2048], P(None, 'tp'), may hold values from -3 to 3
- recur_map: bfloat16 [8, 256, 256], P('tp'), may hold values from -0.375 to 0.375
- input_map: bfloat16 [8, 256, 256], P('tp'), may hold values from -0.375 to 0.375
- rate_logit: float32 [2048], P('tp'), may hold values from 4.5 to 15
- decay_shift: float32 [16384, 8], P('sp', 'tp'), may hold values from -1.5 to 0
- out_weight: bfloat16 [2048, 2048], replicated, may hold values from -0.25 to 0.25
- residual: bfloat16 [16384, 2048], P(('sp', 'tp')), may hold values from -6 to 6
- gain_mix: float32 [2048], replicated, may hold values from 0.1 to 1.9
- routes: int32 [16384, 4], P(('sp', 'tp')), may hold values from 0 to 127, all different within a row; in each aligned block of 128 rows (0 to 127, 128 to 255, ...) at most 8 rows name the same one
- route_weight: float32 [16384, 4], P(('sp', 'tp')), may hold values from 0.2 to 1
- shared_gate: bfloat16 [2048, 512], replicated, may hold values from -0.125 to 0.125
- shared_up: bfloat16 [2048, 512], replicated, may hold values from -0.125 to 0.125
- shared_down: bfloat16 [512, 2048], replicated, may hold values from -0.375 to 0.375
- expert_gate: bfloat16 [128, 2048, 512], P(('sp', 'tp')), may hold values from -0.125 to 0.125
- expert_up: bfloat16 [128, 2048, 512], P(('sp', 'tp')), may hold values from -0.125 to 0.125
- expert_down: bfloat16 [128, 512, 2048], P(('sp', 'tp')), may hold values from -0.375 to 0.375
- gain_out: float32 [2048], replicated, may hold values from 0.1 to 1.9
Outputs:
- layer_out: bfloat16 [16384, 2048], P(('sp', 'tp'))
The draws below stay inside these ranges and needn't reach their ends.
Inputs may be any that keep to these rules, and one draw needn't show every extreme that they name: `routes`: each row names 4 different experts. In the rows of one device (aligned blocks of 128 rows) no expert is named more than 8 times, and in some blocks one expert is named exactly 8 times.
All inputs are finite; a program needn't handle non-finite values.
Results may differ from the reference program's by a relative error of at most 0.014.
Values may be sent and summed in bfloat16 or wider, within the bound.
A program may use at most 128 MiB of HBM per device.

```python
import math
import jax
import jax.numpy as jnp
import numpy as np
from jax import lax

D = 2048
HEADS = 8
BW = 256
DR = 2048
CONV = 4
FE = 512
FS = 512
TOPK = 4
TOKENS_PER_SHARD = 256
TOKENS = 16384
ROWS = 128
EXPERTS = 128
CAP = 8


def draw_rate_logit(key, part):
    flag_key, slow_key, fast_key = jax.random.split(jax.random.fold_in(key, 11), 3)
    fast_share = 0.5
    is_fast = jax.random.uniform(flag_key, (HEADS,), jnp.float32) < fast_share
    slow_rate = jnp.exp(jax.random.uniform(slow_key, (HEADS, BW), jnp.float32, math.log(0.3), math.log(1.2))) / TOKENS
    fast_rate = jnp.exp(jax.random.uniform(fast_key, (HEADS, BW), jnp.float32, math.log(0.02), math.log(0.067)))
    chosen_rate = jnp.where(is_fast[:, None], fast_rate, slow_rate)
    return (-jnp.log(jnp.expm1(chosen_rate / 8.0))).reshape(HEADS * BW).astype(jnp.float32)


def draw_decay_shift(key, part):
    base_key, place_key, size_key = jax.random.split(jax.random.fold_in(key, 23), 3)
    block_count = TOKENS // TOKENS_PER_SHARD
    lowest_value, highest = (0.1, 1.0)
    base = jnp.exp(jax.random.uniform(base_key, (block_count, HEADS), jnp.float32, math.log(lowest_value), math.log(highest))) / TOKENS
    equilibrium_memory = -jnp.repeat(base, TOKENS_PER_SHARD, axis=0)
    location_sequence = jax.random.randint(place_key, (2, HEADS), 0, TOKENS)
    objective_scores = jnp.log(jax.random.uniform(size_key, (2, HEADS), jnp.float32, 0.5, 0.8))
    ordinal_locator = jnp.arange(TOKENS)[:, None]
    arrival_clusters = jnp.where(ordinal_locator == location_sequence[0][None, :], objective_scores[0][None, :], 0.0) + jnp.where(ordinal_locator == location_sequence[1][None, :], objective_scores[1][None, :], 0.0)
    return (equilibrium_memory + arrival_clusters).astype(jnp.float32)


def block_scale(key, extent, cuts, least, top_value):
    def one(position, shards_of):
        steps = jax.random.uniform(jax.random.fold_in(jax.random.fold_in(key, 6), position), (shards_of,), jnp.float32, least / len(cuts), top_value / len(cuts))
        return jnp.repeat(jnp.exp(steps), extent[position] // shards_of).reshape((-1,) + (1,) * (len(extent) - position - 1))

    factor_of = one(*cuts[0])
    for cut in cuts[1:]:
        factor_of = factor_of * one(*cut)
    return factor_of


def assign_block(key, own, number, rows, number_of, top, most, slope):
    ranking = jax.random.permutation(key, number_of)
    packed, common = shares(number_of, rows * top, most, slope, True), shares(number_of, rows * top, most, slope, False)
    places = jnp.arange(number_of)

    def named(tallies, offset_by):
        used = int((tallies > 0).sum())
        fixed = max(1, used // 4)
        passed = fixed + (places - fixed + offset_by * (used - fixed)) % max(1, number_of - fixed)
        return jnp.zeros((number_of,), jnp.int32).at[ranking[jnp.where(places < fixed, places, passed)]].set(jnp.asarray(tallies, jnp.int32))

    tallies = jnp.where(number % 4 == 0, named(packed, number // 4), named(common, number - number // 4 - 1))
    mixed = jax.random.permutation(jax.random.fold_in(own, 3), number_of)
    giver, sink = mixed[0:number_of // 2 * 2:2], mixed[1:number_of // 2 * 2:2]
    slack = jnp.minimum(tallies[giver] - 1, most - tallies[sink]) // 2
    slack = jnp.where((giver == ranking[0]) | (sink == ranking[0]) | (tallies[sink] == 0), 0, jnp.maximum(slack, 0))
    passed = jax.random.randint(jax.random.fold_in(own, 4), (number_of // 2,), 0, 1 << 20) % (slack + 1)
    tallies = tallies.at[giver].add(-passed).at[sink].add(passed)
    labels = jnp.searchsorted(jnp.cumsum(tallies), jnp.arange(rows * top), side="right").astype(jnp.int32)
    listing = labels.reshape(top, rows).T
    listing = listing[jax.random.permutation(jax.random.fold_in(own, 1), rows)]
    offset_by = jax.random.randint(jax.random.fold_in(own, 2), (rows, 1), 0, top)
    return jnp.take_along_axis(listing, (jnp.arange(top)[None, :] + offset_by) % top, axis=1)


def shares(amount, total, bound, slope, full):
    loads = [(1 << 20) // math.isqrt(grade ** slope) + 1 for grade in range(1, amount + 1)]
    largest = bound if full else min(bound, max(-(-total // amount), total * loads[0] // sum(loads)))
    least = 1 if total - largest >= amount - 1 else 0
    given, spare = [largest] + [least] * (amount - 1), total - largest - least * (amount - 1)
    while spare > 0:
        free = [i for i in range(1, amount) if given[i] < largest] or [i for i in range(1, amount) if given[i] < bound]
        mass, left = sum([loads[i] for i in free]), spare
        for i in free:
            addition = min(bound - given[i], max(1, left * loads[i] // mass), spare)
            given[i] = given[i] + addition
            spare = spare - addition
    return np.array(given)


def centred(stream_key, shape, width, reach, cuts=(), kind=jnp.bfloat16):
    gain = block_scale(stream_key, shape, cuts, -0.22, 0.18) if cuts else 1.0
    drawn = jax.random.normal(stream_key, shape, jnp.float32) * width * gain
    return jnp.minimum(jnp.maximum(drawn, -reach), reach).astype(kind)


def setup_inputs(seed: int = 0) -> dict:
    streams_of = jax.random.split(jax.random.key(seed), 20)
    gate_pre = centred(streams_of[0], (TOKENS, DR), 1.0, 6.0, ((0, 64), (1, 2)))
    conv_in = centred(streams_of[1], (TOKENS, DR), 1.0, 6.0, ((0, 64), (1, 2)))
    conv_taps = centred(streams_of[2], (CONV, DR), CONV ** -0.5, 3.0, ((1, 2),))
    recur_map = centred(streams_of[3], (HEADS, BW, BW), BW ** -0.5, 0.375, ((0, 2),))
    input_map = centred(streams_of[4], (HEADS, BW, BW), BW ** -0.5, 0.375, ((0, 2),))
    rate_logit = draw_rate_logit(jax.random.fold_in(streams_of[19], 71), 0)
    decay_shift = draw_decay_shift(jax.random.fold_in(streams_of[19], 71), 0)
    out_weight = centred(streams_of[7], (DR, D), (DR // 4) ** -0.5, 0.25)
    residual = centred(streams_of[8], (TOKENS, D), 1.0, 6.0, ((0, 128),))
    gain_mix = jnp.clip(1.0 + 0.18 * jax.random.normal(streams_of[9], (D,), jnp.float32), 0.1, 1.9)
    routes_keys = jax.random.split(jax.random.fold_in(streams_of[10], 1), TOKENS // ROWS)
    routes_turns = jax.random.permutation(jax.random.fold_in(streams_of[10], 3), TOKENS // ROWS)
    routes = jax.vmap(lambda own, number: assign_block(jax.random.fold_in(streams_of[10], 2), own, number, ROWS, EXPERTS, TOPK, CAP, 1))(routes_keys, routes_turns).reshape((TOKENS, TOPK))
    route_weight = jnp.clip(0.2 + 0.8 * jax.random.uniform(streams_of[11], (TOKENS, TOPK), jnp.float32) ** block_scale(streams_of[11], (TOKENS, TOPK), ((0, 128),), -0.2, 0.2), 0.2, 1.0)
    shared_gate = centred(streams_of[12], (D, FS), D ** -0.5, 0.125)
    shared_up = centred(streams_of[13], (D, FS), D ** -0.5, 0.125)
    shared_down = centred(streams_of[14], (FS, D), (FS // 2) ** -0.5, 0.375)
    expert_gate = centred(streams_of[15], (EXPERTS, D, FE), D ** -0.5, 0.125, ((0, 128),))
    expert_up = centred(streams_of[16], (EXPERTS, D, FE), D ** -0.5, 0.125, ((0, 128),))
    expert_down = centred(streams_of[17], (EXPERTS, FE, D), (FE // 2) ** -0.5, 0.375, ((0, 128),))
    gain_out = jnp.clip(1.0 + 0.18 * jax.random.normal(streams_of[18], (D,), jnp.float32), 0.1, 1.9)
    return dict(gate_pre=gate_pre, conv_in=conv_in, conv_taps=conv_taps, recur_map=recur_map, input_map=input_map, rate_logit=rate_logit, decay_shift=decay_shift, out_weight=out_weight, residual=residual, gain_mix=gain_mix, routes=routes, route_weight=route_weight, shared_gate=shared_gate, shared_up=shared_up, shared_down=shared_down, expert_gate=expert_gate, expert_up=expert_up, expert_down=expert_down, gain_out=gain_out)


ALPHA = 8.0 ** 0.25
RATE_C = 8.0
NORM_EPS = 1e-05

def layer_norm(values, gains):
    center = values - lax.optimization_barrier(jnp.mean(values, axis=-1, keepdims=True))
    spread = lax.optimization_barrier(jnp.mean(center * center, axis=-1, keepdims=True))
    return center * lax.rsqrt(spread + NORM_EPS) * gains

def combine(former, latter):
    return (former[0] * latter[0], latter[0] * former[1] + latter[1])

def reference(gate_pre, conv_in, conv_taps, recur_map, input_map, rate_logit, decay_shift, out_weight, residual, gain_mix, routes, route_weight, shared_gate, shared_up, shared_down, expert_gate, expert_up, expert_down, gain_out):
    length = conv_in.shape[0]
    padded = jnp.concatenate([jnp.zeros((CONV - 1, DR), conv_in.dtype), conv_in], axis=0).astype(jnp.float32)
    filter_tap_weight = conv_taps.astype(jnp.float32)
    summed = jnp.zeros((length, DR), jnp.float32)
    for offset in range(CONV):
        summed = summed + filter_tap_weight[offset] * padded[offset:offset + length]
    conv_out = summed.astype(jnp.bfloat16)
    grouped = conv_out.astype(jnp.float32).reshape(length, HEADS, BW)
    recur_gate = jax.nn.sigmoid(jnp.einsum('thc,hcd->thd', grouped, recur_map.astype(jnp.float32)))
    input_gate = jax.nn.sigmoid(jnp.einsum('thc,hcd->thd', grouped, input_map.astype(jnp.float32)))
    log_decay = -RATE_C * jax.nn.softplus(-rate_logit).reshape(HEADS, BW) * recur_gate + decay_shift[:, :, None]
    update = jnp.sqrt(-jnp.expm1(2.0 * log_decay)) * input_gate * grouped
    states = lax.associative_scan(combine, (jnp.exp(log_decay), update), axis=0)[1]
    mixed_rows = (states.reshape(length, DR) * jax.nn.gelu(gate_pre.astype(jnp.float32), approximate=True)).astype(jnp.bfloat16)
    projected = jnp.dot(mixed_rows, out_weight, preferred_element_type=jnp.float32)
    normed = layer_norm(ALPHA * residual.astype(jnp.float32) + projected, gain_mix).astype(jnp.bfloat16)
    fanout = routes.shape[1]
    flat_ids = routes.reshape(-1).astype(jnp.int32)
    ordering = jnp.argsort(flat_ids, stable=True).astype(jnp.int32)
    sorted_ids = flat_ids[ordering]
    counts = jax.ops.segment_sum(jnp.ones_like(flat_ids), flat_ids, num_segments=EXPERTS).astype(jnp.int32)
    starts = (jnp.cumsum(counts) - counts).astype(jnp.int32)
    within = (jnp.arange(flat_ids.shape[0], dtype=jnp.int32) - starts[sorted_ids]).astype(jnp.int32)
    most_rows = length // ROWS * CAP
    sources = jnp.full((EXPERTS, most_rows), length, jnp.int32).at[sorted_ids, within].set(ordering // fanout)
    weights = jnp.zeros((EXPERTS, most_rows), jnp.float32).at[sorted_ids, within].set(route_weight.reshape(-1)[ordering].astype(jnp.float32))
    padded_rows = jnp.concatenate([normed, jnp.zeros((1, D), jnp.bfloat16)], axis=0)

    def specialist_pass(routed, member):
        chosen_ids, chosen_weights, gate_weight, up_weight, down_weight = member
        chosen = padded_rows[chosen_ids]
        hidden = (jax.nn.silu(jnp.dot(chosen, gate_weight, preferred_element_type=jnp.float32)) * jnp.dot(chosen, up_weight, preferred_element_type=jnp.float32)).astype(jnp.bfloat16)
        result = jnp.dot(hidden, down_weight, preferred_element_type=jnp.float32).astype(jnp.bfloat16)
        return (routed.at[chosen_ids].add(chosen_weights[:, None] * result.astype(jnp.float32)), None)
    routed = lax.scan(specialist_pass, jnp.zeros((length + 1, D), jnp.float32), (sources, weights, expert_gate, expert_up, expert_down))[0]
    shared_hidden = (jax.nn.silu(jnp.dot(normed, shared_gate, preferred_element_type=jnp.float32)) * jnp.dot(normed, shared_up, preferred_element_type=jnp.float32)).astype(jnp.bfloat16)
    moe_sum = jnp.dot(shared_hidden, shared_down, preferred_element_type=jnp.float32) + routed[:length]
    return layer_norm(ALPHA * normed.astype(jnp.float32) + moe_sum, gain_out).astype(jnp.bfloat16)
```

```python
import functools

import jax
import jax.numpy as jnp
from jax import lax
from jax.experimental import pallas as pl
from jax.experimental.pallas import tpu as pltpu
from jax.sharding import PartitionSpec as P

ALPHA = 8.0**0.25
RATE_C = 8.0
NORM_EPS = 1e-05
MESH = pl.DeviceIdType.MESH
F32, BF16 = jnp.float32, jnp.bfloat16

RING = 4
CHUNK = 16
HALO = 16
SPAN = 32


def sigmoid(x):
    return 0.5 * jnp.tanh(0.5 * x) + 0.5


def silu(x):
    return x * sigmoid(x)


def minus_expm1(y):
    series = 1.0 + y * (1.0 / 7.0)
    for n in (6, 5, 4, 3, 2):
        series = 1.0 + (y * (1.0 / n)) * series
    return jnp.where(y > -0.5, -y * series, 1.0 - jnp.exp(y))


def gelu(x):
    inner = 0.7978845608028654 * (x + 0.044715 * (x * x * x))
    return 0.5 * x * (1.0 + jnp.tanh(inner))


def dot(a, b):
    return jnp.dot(a, b, preferred_element_type=F32)


def layer_kernel(
    gate_hbm, conv_hbm, rmap_hbm, imap_hbm, outw_hbm, resid_hbm,
    sgate_hbm, sup_hbm, sdown_hbm, egate_hbm, eup_hbm, edown_hbm,
    taps_ref, rate_ref, shift_ref, gmix_ref, gout_ref,
    routes_ref, routes_t_ref, rw_ref,
    out_ref,
    gate_v, conv_v, rmap_v, imap_v, outw_v, resid_v,
    sgate_v, sup_v, sdown_v, egate_v, eup_v, edown_v,
    halo_v, ext_v, rpre_v, ipre_v, xb_v, a3, u3, g3,
    ca, ch, pa, ph, xbuf, ybuf, zbuf,
    mixed_v, theirs_v, proj_v, normed_v, shared_v, hid_v, rows_v,
    spread_v, merge_v, send_v, recv_v, res_v, ret_v,
    load_sem, halo_sem, line_send, line_recv, pair_sem,
    go_send, go_recv, back_send, back_recv,
):
    sp, tp = lax.axis_index("sp"), lax.axis_index("tp")
    x, y, z = sp % RING, (sp // RING) % RING, sp // (RING * RING)
    peers = RING * RING * RING * 2
    tokens, channels = conv_v.shape
    rows, width = normed_v.shape
    heads, bw = rmap_v.shape[0], rmap_v.shape[1]
    groups = channels // 128

    def offset_of(i):
        core, k = i % 2, i // 2
        a, b, c = k % RING, (k // RING) % RING, k // (RING * RING)
        return core, a, (a + b) % RING, (a + c) % RING

    def device_at(i, sign):
        core, dx, dy, dz = offset_of(i)
        px, py, pz = (
            (w + sign * d + RING) % RING for w, d in ((x, dx), (y, dy), (z, dz))
        )
        return {"sp": (pz * RING + py) * RING + px, "tp": (tp + core) % 2}

    barrier = pltpu.get_barrier_semaphore()

    @pl.loop(1, peers)
    def _(i):
        pl.semaphore_signal(barrier, inc=1, device_id=device_at(i, 1), device_id_type=MESH)

    half = channels
    loads = [
        (conv_hbm, conv_v), (rmap_hbm, rmap_v), (imap_hbm, imap_v), (gate_hbm, gate_v),
        (outw_hbm.at[pl.ds(pl.multiple_of(tp * half, half), half)], outw_v.at[0]),
        (outw_hbm.at[pl.ds(pl.multiple_of((1 - tp) * half, half), half)], outw_v.at[1]),
        (resid_hbm, resid_v),
        (sgate_hbm, sgate_v), (sup_hbm, sup_v), (sdown_hbm, sdown_v),
        (egate_hbm.at[0], egate_v), (eup_hbm.at[0], eup_v), (edown_hbm.at[0], edown_v),
    ]
    loads = [pltpu.make_async_copy(s, d, load_sem.at[n]) for n, (s, d) in enumerate(loads)]
    for copy in loads:
        copy.start()

    loads[0].wait()

    @pl.loop(0, tokens // 32)
    def _(b):
        at = pl.multiple_of(b * 32, 32)
        ext_v[pl.ds(HALO + at, 32), :] = conv_v[pl.ds(at, 32), :].astype(F32)

    loads[1].wait()
    loads[2].wait()

    def gates(first, count, block):
        for h in range(heads):
            cols = pl.ds(h * bw, bw)
            total = None
            for j in range(4):
                term = taps_ref[j : j + 1, cols].astype(F32) * ext_v[
                    pl.ds(HALO + first - 3 + j, count), cols
                ]
                total = term if total is None else total + term
            conv_out = total.astype(BF16)
            xb_v[0:count, :] = conv_out
            rpre_v[0:count, :] = dot(conv_out, rmap_v[h])
            ipre_v[0:count, :] = dot(conv_out, imap_v[h])
            rate = rate_ref[:, cols]

            @pl.loop(0, count // block)
            def _(b):
                at = pl.multiple_of(b * block, block)
                r = sigmoid(rpre_v[pl.ds(at, block), :])
                i = sigmoid(ipre_v[pl.ds(at, block), :])
                where = pl.ds(pl.multiple_of(first + at, 16), block)
                log_decay = rate * r + shift_ref[where, h : h + 1]
                a = jnp.exp(log_decay)
                u = jnp.sqrt(minus_expm1(2.0 * log_decay)) * i * xb_v[pl.ds(at, block), :].astype(F32)
                for g in range(bw // 128):
                    a3[h * (bw // 128) + g, where, :] = a[:, g * 128 : (g + 1) * 128]
                    u3[h * (bw // 128) + g, where, :] = u[:, g * 128 : (g + 1) * 128]

    pl.semaphore_wait(barrier, peers - 1)
    halo = pltpu.make_async_remote_copy(
        src_ref=conv_v.at[pl.ds(tokens - HALO, HALO)], dst_ref=halo_v,
        send_sem=halo_sem.at[0], recv_sem=halo_sem.at[1],
        device_id={"sp": (sp + 1) % (RING * RING * RING), "tp": tp}, device_id_type=MESH,
    )
    halo.start()
    gates(HALO, tokens - HALO, 48)
    halo.wait()
    ext_v[0:HALO, :] = jnp.where(sp == 0, 0.0, halo_v[...].astype(F32))
    gates(0, HALO, 16)

    spans = tokens // SPAN

    def walk(s, carry):
        out = []
        for g in range(groups):
            at = pl.ds(s, spans, stride=SPAN)
            a, u = a3[g, at, :], u3[g, at, :]
            out.append((carry[g][0] * a, a * carry[g][1] + u))
        return tuple(out)

    one, nought = jnp.ones((spans, 128), F32), jnp.zeros((spans, 128), F32)
    ends = lax.fori_loop(0, SPAN, walk, tuple((one, nought) for _ in range(groups)))
    for g in range(groups):
        ca[g * spans : (g + 1) * spans, :] = ends[g][0]
        ch[g * spans : (g + 1) * spans, :] = ends[g][1]
    run_a, run_h = jnp.ones((groups, 128), F32), jnp.zeros((groups, 128), F32)
    for c in range(spans):
        at = pl.ds(c, groups, stride=spans)
        pa[at, :], ph[at, :] = run_a, run_h
        a, h = ca[at, :], ch[at, :]
        run_a, run_h = run_a * a, a * run_h + h

    def exchange(n, buf, here, stride, whole_a, whole_h):
        buf[here, 0:groups, :] = whole_a
        buf[here, groups : 2 * groups, :] = whole_h
        for d in range(1, RING):
            pltpu.make_async_remote_copy(
                src_ref=buf.at[here], dst_ref=buf.at[here],
                send_sem=line_send.at[n], recv_sem=line_recv.at[n],
                device_id={"sp": sp + ((here + d) % RING - here) * stride, "tp": tp},
                device_id_type=MESH,
            ).start()

    def arrived(n, buf):
        three = buf.at[pl.ds(0, RING - 1)]
        copy = pltpu.make_async_remote_copy(
            src_ref=three, dst_ref=three, send_sem=line_send.at[n], recv_sem=line_recv.at[n],
            device_id={"sp": sp, "tp": 1 - tp}, device_id_type=MESH,
        )
        copy.wait_recv()
        copy.wait_send()

    def total_of(buf):
        a, h = buf[0, 0:groups, :], buf[0, groups : 2 * groups, :]
        for n in range(1, RING):
            na, nh = buf[n, 0:groups, :], buf[n, groups : 2 * groups, :]
            a, h = a * na, na * h + nh
        return a, h

    exchange(0, xbuf, x, 1, run_a, run_h)

    loads[3].wait()

    @pl.loop(0, tokens // 32)
    def _(b):
        at = pl.multiple_of(b * 32, 32)
        for g in range(groups):
            g3[g, pl.ds(at, 32), :] = gelu(gate_v[pl.ds(at, 32), g * 128 : (g + 1) * 128].astype(F32))

    arrived(0, xbuf)
    exchange(1, ybuf, y, RING, *total_of(xbuf))

    slots = 8
    lane_e = lax.broadcasted_iota(jnp.int32, (rows, peers), 1)
    sub_e = lax.broadcasted_iota(jnp.int32, (peers, rows), 0)
    member, member_t = jnp.zeros((rows, peers), F32), jnp.zeros((peers, rows), F32)
    weight = jnp.zeros((rows, peers), F32)
    for k in range(4):
        hit = routes_ref[:, k : k + 1] == lane_e
        member = member + jnp.where(hit, 1.0, 0.0)
        weight = weight + jnp.where(hit, rw_ref[:, k : k + 1], 0.0)
        member_t = member_t + jnp.where(routes_t_ref[k : k + 1, :] == sub_e, 1.0, 0.0)
    i0 = lax.broadcasted_iota(jnp.int32, (rows, rows), 0)
    i1 = lax.broadcasted_iota(jnp.int32, (rows, rows), 1)
    below = jnp.where(i0 > i1, 1.0, 0.0).astype(BF16)
    above = jnp.where(i0 < i1, 1.0, 0.0).astype(BF16)
    place = ((dot(below, member.astype(BF16)) + 1.0) * member).astype(BF16)
    place_t = ((dot(member_t.astype(BF16), above) + 1.0) * member_t).astype(BF16)
    weight_hi = weight.astype(BF16)
    weight_lo = (weight - weight_hi.astype(F32)).astype(BF16)

    def expert_of(i):
        core, dx, dy, dz = offset_of(i)
        chip = (((z + dz) % RING) * RING + (y + dy) % RING) * RING + (x + dx) % RING
        return chip * 2 + (tp + core) % 2

    for q in range(peers * slots // 256):
        r0 = lax.broadcasted_iota(jnp.int32, (256, peers), 0) + q * 256
        pick = jnp.where(
            expert_of(r0 // slots) == lax.broadcasted_iota(jnp.int32, (256, peers), 1), 1.0, 0.0
        ).astype(BF16)
        found = dot(pick, place_t)
        slot = (lax.broadcasted_iota(jnp.int32, (256, rows), 0) % slots + 1).astype(F32)
        spread_v[q * 256 : (q + 1) * 256, :] = jnp.where(found == slot, 1.0, 0.0).astype(BF16)
        r1 = lax.broadcasted_iota(jnp.int32, (peers, 256), 1) + q * 256
        pick_t = jnp.where(
            expert_of(r1 // slots) == lax.broadcasted_iota(jnp.int32, (peers, 256), 0), 1.0, 0.0
        ).astype(BF16)
        slot_t = (lax.broadcasted_iota(jnp.int32, (rows, 256), 1) % slots + 1).astype(F32)
        match = dot(place, pick_t) == slot_t
        merge_v[q, 0:rows, :] = jnp.where(match, dot(weight_hi, pick_t), 0.0).astype(BF16)
        merge_v[q, rows : 2 * rows, :] = jnp.where(match, dot(weight_lo, pick_t), 0.0).astype(BF16)

    arrived(1, ybuf)
    exchange(2, zbuf, z, RING * RING, *total_of(ybuf))
    arrived(2, zbuf)

    state = jnp.zeros((groups, 128), F32)
    for buf, here in ((zbuf, z), (ybuf, y), (xbuf, x)):
        for n in range(RING - 1):
            a, h = buf[n, 0:groups, :], buf[n, groups : 2 * groups, :]
            state = jnp.where(n < here, a * state + h, state)

    starts = tuple(
        pa[g * spans : (g + 1) * spans, :] * state[g : g + 1, :] + ph[g * spans : (g + 1) * spans, :]
        for g in range(groups)
    )

    def rewalk(s, carry):
        out = []
        for g in range(groups):
            at = pl.ds(s, spans, stride=SPAN)
            h = a3[g, at, :] * carry[g] + u3[g, at, :]
            u3[g, at, :] = h * g3[g, at, :]
            out.append(h)
        return tuple(out)

    lax.fori_loop(0, SPAN, rewalk, starts)

    @pl.loop(0, tokens // 32)
    def _(b):
        at = pl.multiple_of(b * 32, 32)
        for g in range(groups):
            mixed_v[pl.ds(at, 32), g * 128 : (g + 1) * 128] = u3[g, pl.ds(at, 32), :].astype(BF16)

    pair = pltpu.make_async_remote_copy(
        src_ref=mixed_v.at[pl.ds(pl.multiple_of((1 - tp) * rows, rows), rows)], dst_ref=theirs_v,
        send_sem=pair_sem.at[0], recv_sem=pair_sem.at[1],
        device_id={"sp": sp, "tp": 1 - tp}, device_id_type=MESH,
    )
    pair.start()

    tile = 256
    mine = mixed_v[pl.ds(pl.multiple_of(tp * rows, rows), rows), :]
    loads[4].wait()

    @pl.loop(0, width // tile)
    def _(n):
        cols = pl.ds(pl.multiple_of(n * tile, tile), tile)
        proj_v[:, cols] = dot(mine, outw_v[0, :, cols])

    loads[5].wait()
    loads[6].wait()
    pair.wait()
    theirs = theirs_v[...]

    @pl.loop(0, width // tile)
    def _(n):
        cols = pl.ds(pl.multiple_of(n * tile, tile), tile)
        proj_v[:, cols] = (
            ALPHA * resid_v[:, cols].astype(F32) + proj_v[:, cols] + dot(theirs, outw_v[1, :, cols])
        )

    def layer_norm(values, gains):
        center = values - jnp.mean(values, axis=-1, keepdims=True)
        spread = jnp.mean(center * center, axis=-1, keepdims=True)
        return center * lax.rsqrt(spread + NORM_EPS) * gains

    @pl.loop(0, rows // 16)
    def _(b):
        at = pl.ds(pl.multiple_of(b * 16, 16), 16)
        normed_v[at, :] = layer_norm(proj_v[at, :], gmix_ref[...]).astype(BF16)

    chunks = peers // CHUNK
    block = CHUNK * slots

    def chunk_of(ref, j):
        return ref.at[pl.ds(pl.multiple_of(j * CHUNK, CHUNK), CHUNK)]

    @pl.loop(0, chunks)
    def _(j):
        pick = spread_v[pl.ds(pl.multiple_of(j * block, block), block), :]
        for n in range(width // 512):
            part = dot(pick, normed_v[:, n * 512 : (n + 1) * 512])
            send_v[pl.ds(j * CHUNK, CHUNK), :, n * 512 : (n + 1) * 512] = part.reshape(
                CHUNK, slots, 512
            ).astype(BF16)

        @pl.loop(jnp.where(j == 0, 1, 0), CHUNK)
        def _(i):
            at = j * CHUNK + i
            pltpu.make_async_remote_copy(
                src_ref=send_v.at[at], dst_ref=recv_v.at[at],
                send_sem=go_send.at[j], recv_sem=go_recv.at[j],
                device_id=device_at(at, 1), device_id_type=MESH,
            ).start()

    def expert(x_in, gate, up, down, store):
        @pl.loop(0, gate.shape[1] // tile)
        def _(n):
            cols = pl.ds(pl.multiple_of(n * tile, tile), tile)
            hid_v[:, cols] = (silu(dot(x_in, gate[:, cols])) * dot(x_in, up[:, cols])).astype(BF16)

        hidden = hid_v[...]

        @pl.loop(0, width // tile)
        def _(n):
            cols = pl.ds(pl.multiple_of(n * tile, tile), tile)
            store(cols, dot(hidden, down[:, cols]))

    def keep_shared(cols, value):
        shared_v[:, cols] = ALPHA * normed_v[:, cols].astype(F32) + value

    loads[7].wait()
    loads[8].wait()
    loads[9].wait()
    expert(normed_v[...], sgate_v, sup_v, sdown_v, keep_shared)
    loads[10].wait()
    loads[11].wait()
    loads[12].wait()

    def waiter(ref, send, recv, j, first):
        part = ref.at[pl.ds(pl.multiple_of(j * CHUNK, CHUNK) + first, CHUNK - first)]
        return pltpu.make_async_remote_copy(
            src_ref=part, dst_ref=part, send_sem=send.at[j], recv_sem=recv.at[j],
            device_id={"sp": sp, "tp": 1 - tp}, device_id_type=MESH,
        )

    def serve(j, first):
        waiter(recv_v, go_send, go_recv, j, first).wait_recv()
        chosen = recv_v[pl.ds(j * CHUNK, CHUNK)]
        rows_v[...] = chosen.astype(F32).reshape(block, width).astype(BF16)

        def give(cols, value):
            res_v[pl.ds(j * CHUNK, CHUNK), :, cols] = value.reshape(CHUNK, slots, tile).astype(BF16)

        expert(rows_v[...], egate_v, eup_v, edown_v, give)

        @pl.loop(first, CHUNK)
        def _(i):
            at = j * CHUNK + i
            pltpu.make_async_remote_copy(
                src_ref=res_v.at[at], dst_ref=ret_v.at[at],
                send_sem=back_send.at[j], recv_sem=back_recv.at[j],
                device_id=device_at(at, -1), device_id_type=MESH,
            ).start()

    recv_v[0] = send_v[0]
    serve(0, 1)
    ret_v[0] = res_v[0]

    @pl.loop(1, chunks)
    def _(j):
        serve(j, 0)

    def merge(q, first):
        waiter(ret_v, back_send, back_recv, 2 * q, first).wait_recv()
        waiter(ret_v, back_send, back_recv, 2 * q + 1, 0).wait_recv()
        share = merge_v[q]

        @pl.loop(0, width // tile)
        def _(n):
            cols = pl.ds(pl.multiple_of(n * tile, tile), tile)
            back = ret_v[pl.ds(2 * q * CHUNK, 2 * CHUNK), :, cols]
            back = back.astype(F32).reshape(2 * block, tile).astype(BF16)
            both = dot(share, back)
            shared_v[:, cols] += both[0:rows] + both[rows : 2 * rows]

    merge(0, 1)

    @pl.loop(1, chunks // 2)
    def _(q):
        merge(q, 0)

    @pl.loop(0, rows // 16)
    def _(b):
        at = pl.ds(pl.multiple_of(b * 16, 16), 16)
        out_ref[at, :] = layer_norm(shared_v[at, :], gout_ref[...]).astype(BF16)

    waiter(send_v, go_send, go_recv, 0, 1).wait_send()
    waiter(res_v, back_send, back_recv, 0, 1).wait_send()

    @pl.loop(1, chunks)
    def _(j):
        waiter(send_v, go_send, go_recv, j, 0).wait_send()
        waiter(res_v, back_send, back_recv, j, 0).wait_send()


def on_device(
    gate_pre, conv_in, conv_taps, recur_map, input_map, rate_logit, decay_shift, out_weight,
    residual, gain_mix, routes, route_weight, shared_gate, shared_up, shared_down,
    expert_gate, expert_up, expert_down, gain_out,
):
    tokens, channels = conv_in.shape
    rows, width = residual.shape
    heads, bw = recur_map.shape[:2]
    hidden = shared_gate.shape[1]
    groups, spans, peers, slots = channels // 128, tokens // SPAN, 2 * RING**3, 8
    rate = (-RATE_C * jax.nn.softplus(-rate_logit)).reshape(1, channels)
    any_spec = pl.BlockSpec(memory_space=pl.ANY)
    vmem_spec = pl.BlockSpec(memory_space=pltpu.VMEM)
    big = [
        gate_pre, conv_in, recur_map, input_map, out_weight, residual,
        shared_gate, shared_up, shared_down, expert_gate, expert_up, expert_down,
    ]
    small = [
        conv_taps, rate, decay_shift, gain_mix.reshape(1, width), gain_out.reshape(1, width),
        routes, routes.T, route_weight,
    ]
    dma = pltpu.SemaphoreType.DMA
    chunks = peers // CHUNK
    return pl.pallas_call(
        layer_kernel,
        out_shape=jax.ShapeDtypeStruct((rows, width), BF16),
        in_specs=[any_spec] * len(big) + [vmem_spec] * len(small),
        out_specs=vmem_spec,
        scratch_shapes=[
            pltpu.VMEM((tokens, channels), BF16),
            pltpu.VMEM((tokens, channels), BF16),
            pltpu.VMEM((heads, bw, bw), BF16),
            pltpu.VMEM((heads, bw, bw), BF16),
            pltpu.VMEM((2, channels, width), BF16),
            pltpu.VMEM((rows, width), BF16),
            pltpu.VMEM((width, hidden), BF16),
            pltpu.VMEM((width, hidden), BF16),
            pltpu.VMEM((hidden, width), BF16),
            pltpu.VMEM((width, hidden), BF16),
            pltpu.VMEM((width, hidden), BF16),
            pltpu.VMEM((hidden, width), BF16),
            pltpu.VMEM((HALO, channels), BF16),
            pltpu.VMEM((HALO + tokens, channels), F32),
            pltpu.VMEM((tokens, bw), F32),
            pltpu.VMEM((tokens, bw), F32),
            pltpu.VMEM((tokens, bw), BF16),
            pltpu.VMEM((groups, tokens, 128), F32),
            pltpu.VMEM((groups, tokens, 128), F32),
            pltpu.VMEM((groups, tokens, 128), F32),
            pltpu.VMEM((groups * spans, 128), F32),
            pltpu.VMEM((groups * spans, 128), F32),
            pltpu.VMEM((groups * spans, 128), F32),
            pltpu.VMEM((groups * spans, 128), F32),
            pltpu.VMEM((RING, 2 * groups, 128), F32),
            pltpu.VMEM((RING, 2 * groups, 128), F32),
            pltpu.VMEM((RING, 2 * groups, 128), F32),
            pltpu.VMEM((tokens, channels), BF16),
            pltpu.VMEM((rows, channels), BF16),
            pltpu.VMEM((rows, width), F32),
            pltpu.VMEM((rows, width), BF16),
            pltpu.VMEM((rows, width), F32),
            pltpu.VMEM((CHUNK * slots, hidden), BF16),
            pltpu.VMEM((CHUNK * slots, width), BF16),
            pltpu.VMEM((peers * slots, rows), BF16),
            pltpu.VMEM((chunks // 2, 2 * rows, 2 * CHUNK * slots), BF16),
            pltpu.VMEM((peers, slots, width), BF16),
            pltpu.VMEM((peers, slots, width), BF16),
            pltpu.VMEM((peers, slots, width), BF16),
            pltpu.VMEM((peers, slots, width), BF16),
            dma((13,)), dma((2,)), dma((3,)), dma((3,)), dma((2,)),
            dma((chunks,)), dma((chunks,)), dma((chunks,)), dma((chunks,)),
        ],
        compiler_params=pltpu.CompilerParams(
            collective_id=0, has_side_effects=True, vmem_limit_bytes=67_043_328 - 2 * 1024 * 1024
        ),
        name="layer",
    )(*big, *small)


def solution(mesh):
    return jax.shard_map(
        on_device,
        mesh=mesh,
        in_specs=(
            P("sp", "tp"), P("sp", "tp"), P(None, "tp"), P("tp", None, None), P("tp", None, None),
            P("tp"), P("sp", "tp"), P(), P(("sp", "tp"), None), P(), P(("sp", "tp"), None),
            P(("sp", "tp"), None), P(), P(), P(), P(("sp", "tp"), None, None),
            P(("sp", "tp"), None, None), P(("sp", "tp"), None, None), P(),
        ),
        out_specs=P(("sp", "tp"), None),
        check_vma=False,
    )
```

```python
import functools

import jax
import jax.numpy as jnp
from jax import lax
from jax.experimental import pallas as pl
from jax.experimental.pallas import tpu as pltpu
from jax.sharding import PartitionSpec as P

ALPHA = 8.0**0.25
RATE_C = 8.0
NORM_EPS = 1e-05
MESH = pl.DeviceIdType.MESH
F32, BF16 = jnp.float32, jnp.bfloat16

RING = 4
CHUNK = 16
HALO = 16
SPAN = 32
PITCH = 40


def sigmoid(x):
    return 0.5 * jnp.tanh(0.5 * x) + 0.5


def silu(x):
    return x * sigmoid(x)


def minus_expm1(y):
    series = 1.0 + y * (1.0 / 7.0)
    for n in (6, 5, 4, 3, 2):
        series = 1.0 + (y * (1.0 / n)) * series
    return jnp.where(y > -0.5, -y * series, 1.0 - jnp.exp(y))


def gelu(x):
    inner = 0.7978845608028654 * (x + 0.044715 * (x * x * x))
    return 0.5 * x * (1.0 + jnp.tanh(inner))


def softplus(v):
    tail = jnp.exp(-jnp.abs(v))
    s = tail / (2.0 + tail)
    q = s * s
    series = 1.0 / 17.0
    for n in (15, 13, 11, 9, 7, 5, 3):
        series = 1.0 / n + q * series
    return jnp.maximum(v, 0.0) + 2.0 * s * (1.0 + q * series)


def dot(a, b):
    return jnp.dot(a, b, preferred_element_type=F32)


def layer_kernel(
    gate_hbm, conv_hbm, rmap_hbm, imap_hbm, outw_hbm, resid_hbm,
    sgate_hbm, sup_hbm, sdown_hbm, egate_hbm, eup_hbm, edown_hbm,
    taps_hbm, logit_hbm, shift_hbm, gmix_hbm, gout_hbm, routes_hbm, rw_hbm,
    out_ref,
    taps_ref, logit_ref, shift_t_ref, gmix_ref, gout_ref, routes_t_ref, rw_t_ref, shift_ref,
    gate_v, conv_v, rmap_v, imap_v, outw_v, resid_v,
    sgate_v, sup_v, sdown_v, egate_v, eup_v, edown_v,
    halo_v, ext_v, rpre_v, ipre_v, xb_v, a3, u3, g3,
    ca, ch, pa, ph, plane_buf, zbuf,
    mixed_v, theirs_v, proj_v, normed_v, shared_v, hid_v, rows_v,
    spread_v, merge_v, send_v, recv_v, res_v, ret_v,
    load_sem, halo_sem, line_send, line_recv, pair_sem,
    go_send, go_recv, back_send, back_recv,
):
    sp, tp = lax.axis_index("sp"), lax.axis_index("tp")
    x, y, z = sp % RING, (sp // RING) % RING, sp // (RING * RING)
    peers = RING * RING * RING * 2
    tokens, channels = conv_v.shape
    rows, width = normed_v.shape
    heads, bw = rmap_v.shape[0], rmap_v.shape[1]
    groups = channels // 128

    def wrap(v):
        return lax.rem(v, RING)

    def partners(m, sign):
        b, c = wrap(m), lax.div(m, RING)
        for a in range(RING):
            px = wrap(x + sign * a + RING)
            py = wrap(y + sign * (a + b) + 2 * RING)
            pz = wrap(z + sign * (a + c) + 2 * RING)
            for core in range(2):
                other = tp if core == 0 else 1 - tp
                yield a * 2 + core, {"sp": (pz * RING + py) * RING + px, "tp": other}

    def to_partners(m, sign, act):
        for n, device in partners(m, sign):
            if n == 0:

                @pl.when(m > 0)
                def _():
                    act(m * 8, device)

            else:
                act(m * 8 + n, device)

    def offset_of(i):
        core, k = i % 2, i // 2
        a, b, c = k % RING, (k // RING) % RING, k // (RING * RING)
        return core, a, (a + b) % RING, (a + c) % RING

    barrier = pltpu.get_barrier_semaphore()

    half = channels
    loads = [
        (conv_hbm, conv_v), (rmap_hbm, rmap_v), (imap_hbm, imap_v), (gate_hbm, gate_v),
        (outw_hbm.at[pl.ds(pl.multiple_of(tp * half, half), half)], outw_v.at[0]),
        (outw_hbm.at[pl.ds(pl.multiple_of((1 - tp) * half, half), half)], outw_v.at[1]),
        (resid_hbm, resid_v),
        (sgate_hbm, sgate_v), (sup_hbm, sup_v), (sdown_hbm, sdown_v),
        (egate_hbm.at[0], egate_v), (eup_hbm.at[0], eup_v), (edown_hbm.at[0], edown_v),
        (taps_hbm, taps_ref), (logit_hbm, logit_ref), (shift_hbm, shift_t_ref),
        (routes_hbm, routes_t_ref), (rw_hbm, rw_t_ref), (gmix_hbm, gmix_ref), (gout_hbm, gout_ref),
    ]
    loads = [pltpu.make_async_copy(s, d, load_sem.at[n]) for n, (s, d) in enumerate(loads)]
    for copy in loads[0:1] + loads[13:16] + loads[1:4] + loads[16:] + loads[4:13]:
        copy.start()

    @pl.loop(0, peers // 8)
    def _(m):
        def greet(at, device):
            pl.semaphore_signal(barrier, inc=1, device_id=device, device_id_type=MESH)

        to_partners(m, 1, greet)

    loads[0].wait()

    @pl.loop(0, tokens // 32)
    def _(b):
        at = pl.multiple_of(b * 32, 32)
        ext_v[pl.ds(HALO + at, 32), :] = conv_v[pl.ds(at, 32), :].astype(F32)

    for n in (13, 14, 15, 1, 2):
        loads[n].wait()
    rate = -RATE_C * softplus(-logit_ref[...])
    shift_rows = jnp.concatenate([shift_t_ref[...], jnp.zeros_like(shift_t_ref[...])], axis=0)
    shift_ref[...] = shift_rows.T

    def gates(h, first, count):
        cols = slice(h * bw, (h + 1) * bw)
        total = None
        for j in range(4):
            term = taps_ref[j : j + 1, cols].astype(F32) * ext_v[
                pl.ds(HALO + first - 3 + j, count), cols
            ]
            total = term if total is None else total + term
        conv_out = total.astype(BF16)
        xb_v[0:count, :] = conv_out
        rpre_v[0:count, :] = dot(conv_out, rmap_v[h])
        ipre_v[0:count, :] = dot(conv_out, imap_v[h])

        @pl.loop(0, count // SPAN)
        def _(b):
            at = pl.ds(pl.multiple_of(b * SPAN, SPAN), SPAN)
            r = sigmoid(rpre_v[at, :])
            i = sigmoid(ipre_v[at, :])
            shift = shift_ref[pl.ds(pl.multiple_of(first + b * SPAN, SPAN), SPAN), h : h + 1]
            log_decay = rate[:, cols] * r + shift
            a = jnp.exp(log_decay)
            u = jnp.sqrt(minus_expm1(2.0 * log_decay)) * i * xb_v[at, :].astype(F32)
            keep = pl.ds(pl.multiple_of((first // SPAN + b) * PITCH, 8), SPAN)
            for g in range(bw // 128):
                a3[h * (bw // 128) + g, keep, :] = a[:, g * 128 : (g + 1) * 128]
                u3[h * (bw // 128) + g, keep, :] = u[:, g * 128 : (g + 1) * 128]

    for h in range(heads // 2):
        gates(h, SPAN, tokens - SPAN)
    pl.semaphore_wait(barrier, peers - 1)
    halo = pltpu.make_async_remote_copy(
        src_ref=conv_v.at[pl.ds(tokens - HALO, HALO)], dst_ref=halo_v,
        send_sem=halo_sem.at[0], recv_sem=halo_sem.at[1],
        device_id={"sp": lax.rem(sp + 1, RING * RING * RING), "tp": tp}, device_id_type=MESH,
    )
    halo.start()
    for h in range(heads // 2, heads):
        gates(h, SPAN, tokens - SPAN)

    loads[3].wait()

    @pl.loop(0, tokens // SPAN)
    def _(b):
        at = pl.multiple_of(b * SPAN, SPAN)
        for g in range(groups):
            g3[g, pl.ds(pl.multiple_of(b * PITCH, 8), SPAN), :] = gelu(
                gate_v[pl.ds(at, SPAN), g * 128 : (g + 1) * 128].astype(F32)
            )

    halo.wait()
    ext_v[0:HALO, :] = jnp.where(sp == 0, 0.0, halo_v[...].astype(F32))
    for h in range(heads):
        gates(h, 0, SPAN)

    spans = tokens // SPAN

    def walk(s, carry):
        out = []
        for g in range(groups):
            at = pl.ds(s, spans, stride=PITCH)
            a, u = a3[g, at, :], u3[g, at, :]
            out.append((carry[g][0] * a, a * carry[g][1] + u))
        return tuple(out)

    one, nought = jnp.ones((spans, 128), F32), jnp.zeros((spans, 128), F32)
    ends = lax.fori_loop(0, SPAN, walk, tuple((one, nought) for _ in range(groups)), unroll=4)
    for g in range(groups):
        ca[g * spans : (g + 1) * spans, :] = ends[g][0]
        ch[g * spans : (g + 1) * spans, :] = ends[g][1]
    run_a, run_h = jnp.ones((groups, 128), F32), jnp.zeros((groups, 128), F32)
    for c in range(spans):
        at = pl.ds(c, groups, stride=spans)
        pa[at, :], ph[at, :] = run_a, run_h
        a, h = ca[at, :], ch[at, :]
        run_a, run_h = run_a * a, a * run_h + h

    def exchange(n, buf, here, stride, whole_a, whole_h):
        count = buf.shape[0]
        buf[here, 0:groups, :] = whole_a
        buf[here, groups : 2 * groups, :] = whole_h

        @pl.loop(1, count)
        def _(d):
            pltpu.make_async_remote_copy(
                src_ref=buf.at[here], dst_ref=buf.at[here],
                send_sem=line_send.at[n], recv_sem=line_recv.at[n],
                device_id={"sp": sp + (lax.rem(here + d, count) - here) * stride, "tp": tp},
                device_id_type=MESH,
            ).start()

    def arrived(n, buf):
        others = buf.at[pl.ds(0, buf.shape[0] - 1)]
        copy = pltpu.make_async_remote_copy(
            src_ref=others, dst_ref=others, send_sem=line_send.at[n], recv_sem=line_recv.at[n],
            device_id={"sp": sp, "tp": 1 - tp}, device_id_type=MESH,
        )
        copy.wait_recv()
        copy.wait_send()

    in_plane = y * RING + x
    exchange(0, plane_buf, in_plane, 1, run_a, run_h)

    loads[16].wait()
    loads[17].wait()
    slots = 8
    sub_e = lax.broadcasted_iota(jnp.int32, (peers, rows), 0)
    member_t, weight_t = jnp.zeros((peers, rows), F32), jnp.zeros((peers, rows), F32)
    for k in range(4):
        hit = routes_t_ref[k : k + 1, :] == sub_e
        member_t = member_t + jnp.where(hit, 1.0, 0.0)
        weight_t = weight_t + jnp.where(hit, rw_t_ref[k : k + 1, :], 0.0)
    i0 = lax.broadcasted_iota(jnp.int32, (rows, rows), 0)
    i1 = lax.broadcasted_iota(jnp.int32, (rows, rows), 1)
    above = jnp.where(i0 < i1, 1.0, 0.0).astype(BF16)
    ranks_t = (dot(member_t.astype(BF16), above) + 1.0) * member_t
    place_t = ranks_t.astype(BF16)
    place = ranks_t.T.astype(BF16)
    weight = weight_t.T
    weight_hi = weight.astype(BF16)
    weight_lo = (weight - weight_hi.astype(F32)).astype(BF16)

    def expert_of(i):
        core, dx, dy, dz = offset_of(i)
        chip = (((z + dz) % RING) * RING + (y + dy) % RING) * RING + (x + dx) % RING
        return chip * 2 + (tp + core) % 2

    wide = 256
    slot = (lax.broadcasted_iota(jnp.int32, (wide, rows), 0) % slots + 1).astype(F32)
    slot_t = (lax.broadcasted_iota(jnp.int32, (rows, wide), 1) % slots + 1).astype(F32)
    step_i = lax.broadcasted_iota(jnp.int32, (wide, 1), 0)
    step_t = lax.broadcasted_iota(jnp.int32, (1, wide), 1)
    name_i = lax.broadcasted_iota(jnp.int32, (wide, peers), 1)
    name_t = lax.broadcasted_iota(jnp.int32, (peers, wide), 0)
    for q in range(peers * slots // wide):
        pick = jnp.where(expert_of((step_i + q * wide) // slots) == name_i, 1.0, 0.0).astype(BF16)
        found = dot(pick, place_t)
        spread_v[q * wide : (q + 1) * wide, :] = jnp.where(found == slot, 1.0, 0.0).astype(BF16)

    arrived(0, plane_buf)
    plane_a, plane_h = plane_buf[0, 0:groups, :], plane_buf[0, groups : 2 * groups, :]
    for n in range(1, RING * RING):
        a, h = plane_buf[n, 0:groups, :], plane_buf[n, groups : 2 * groups, :]
        plane_a, plane_h = plane_a * a, plane_h * a + h
    exchange(1, zbuf, z, RING * RING, plane_a, plane_h)
    for q in range(peers * slots // wide):
        pick_t = jnp.where(expert_of((step_t + q * wide) // slots) == name_t, 1.0, 0.0).astype(BF16)
        match = dot(place, pick_t) == slot_t
        merge_v[q, 0:rows, :] = jnp.where(match, dot(weight_hi, pick_t), 0.0).astype(BF16)
        merge_v[q, rows : 2 * rows, :] = jnp.where(match, dot(weight_lo, pick_t), 0.0).astype(BF16)

    arrived(1, zbuf)

    state = jnp.zeros((groups, 128), F32)
    for buf, here in ((zbuf, z), (plane_buf, in_plane)):
        for n in range(buf.shape[0] - 1):
            a, h = buf[n, 0:groups, :], buf[n, groups : 2 * groups, :]
            state = jnp.where(n < here, a * state + h, state)

    starts = tuple(
        pa[g * spans : (g + 1) * spans, :] * state[g : g + 1, :] + ph[g * spans : (g + 1) * spans, :]
        for g in range(groups)
    )

    def rewalk(s, carry):
        out = []
        for g in range(groups):
            at = pl.ds(s, spans, stride=PITCH)
            h = a3[g, at, :] * carry[g] + u3[g, at, :]
            u3[g, at, :] = h * g3[g, at, :]
            out.append(h)
        return tuple(out)

    lax.fori_loop(0, SPAN, rewalk, starts, unroll=4)

    def round_rows(first):
        @pl.loop(0, rows // SPAN)
        def _(b):
            at = pl.ds(pl.multiple_of(first + b * SPAN, SPAN), SPAN)
            keep = pl.ds(pl.multiple_of((first // SPAN + b) * PITCH, 8), SPAN)
            for g in range(groups):
                mixed_v[at, g * 128 : (g + 1) * 128] = u3[g, keep, :].astype(BF16)

    round_rows((1 - tp) * rows)
    pair = pltpu.make_async_remote_copy(
        src_ref=mixed_v.at[pl.ds(pl.multiple_of((1 - tp) * rows, rows), rows)], dst_ref=theirs_v,
        send_sem=pair_sem.at[0], recv_sem=pair_sem.at[1],
        device_id={"sp": sp, "tp": 1 - tp}, device_id_type=MESH,
    )
    pair.start()
    round_rows(tp * rows)

    tile = 256
    mine = mixed_v[pl.ds(pl.multiple_of(tp * rows, rows), rows), :]
    loads[4].wait()

    @pl.loop(0, width // tile)
    def _(n):
        cols = pl.ds(pl.multiple_of(n * tile, tile), tile)
        proj_v[:, cols] = dot(mine, outw_v[0, :, cols])

    loads[5].wait()
    loads[6].wait()
    pair.wait()
    theirs = theirs_v[...]

    @pl.loop(0, width // tile)
    def _(n):
        cols = pl.ds(pl.multiple_of(n * tile, tile), tile)
        proj_v[:, cols] = (
            ALPHA * resid_v[:, cols].astype(F32) + proj_v[:, cols] + dot(theirs, outw_v[1, :, cols])
        )

    def layer_norm(values, gains):
        center = values - jnp.mean(values, axis=-1, keepdims=True)
        spread = jnp.mean(center * center, axis=-1, keepdims=True)
        return center * lax.rsqrt(spread + NORM_EPS) * gains

    loads[18].wait()
    loads[19].wait()

    @pl.loop(0, rows // 16)
    def _(b):
        at = pl.ds(pl.multiple_of(b * 16, 16), 16)
        normed_v[at, :] = layer_norm(proj_v[at, :], gmix_ref[...]).astype(BF16)

    chunks = peers // CHUNK
    block = CHUNK * slots

    def chunk_of(ref, j):
        return ref.at[pl.ds(pl.multiple_of(j * CHUNK, CHUNK), CHUNK)]

    @pl.loop(0, chunks)
    def _(j):
        pick = spread_v[pl.ds(pl.multiple_of(j * block, block), block), :]
        for n in range(width // 512):
            part = dot(pick, normed_v[:, n * 512 : (n + 1) * 512])
            send_v[pl.ds(j * CHUNK, CHUNK), :, n * 512 : (n + 1) * 512] = part.reshape(
                CHUNK, slots, 512
            ).astype(BF16)

        def give(at, device):
            pltpu.make_async_remote_copy(
                src_ref=send_v.at[at], dst_ref=recv_v.at[at],
                send_sem=go_send.at[j], recv_sem=go_recv.at[j],
                device_id=device, device_id_type=MESH,
            ).start()

        @pl.loop(0, CHUNK // 8)
        def _(half):
            to_partners(j * (CHUNK // 8) + half, 1, give)

    def expert(x_in, gate, up, down, store):
        @pl.loop(0, gate.shape[1] // tile)
        def _(n):
            cols = pl.ds(pl.multiple_of(n * tile, tile), tile)
            hid_v[:, cols] = (silu(dot(x_in, gate[:, cols])) * dot(x_in, up[:, cols])).astype(BF16)

        hidden = hid_v[...]

        @pl.loop(0, width // tile)
        def _(n):
            cols = pl.ds(pl.multiple_of(n * tile, tile), tile)
            store(cols, dot(hidden, down[:, cols]))

    def keep_shared(cols, value):
        shared_v[:, cols] = ALPHA * normed_v[:, cols].astype(F32) + value

    loads[7].wait()
    loads[8].wait()
    loads[9].wait()
    expert(normed_v[...], sgate_v, sup_v, sdown_v, keep_shared)
    loads[10].wait()
    loads[11].wait()
    loads[12].wait()

    def waiter(ref, send, recv, j, first):
        part = ref.at[pl.ds(pl.multiple_of(j * CHUNK, CHUNK) + first, CHUNK - first)]
        return pltpu.make_async_remote_copy(
            src_ref=part, dst_ref=part, send_sem=send.at[j], recv_sem=recv.at[j],
            device_id={"sp": sp, "tp": 1 - tp}, device_id_type=MESH,
        )

    def serve(j, first):
        waiter(recv_v, go_send, go_recv, j, first).wait_recv()
        chosen = recv_v[pl.ds(j * CHUNK, CHUNK)]
        rows_v[...] = chosen.astype(F32).reshape(block, width).astype(BF16)

        def give(cols, value):
            res_v[pl.ds(j * CHUNK, CHUNK), :, cols] = value.reshape(CHUNK, slots, tile).astype(BF16)

        expert(rows_v[...], egate_v, eup_v, edown_v, give)

        def give_back(at, device):
            pltpu.make_async_remote_copy(
                src_ref=res_v.at[at], dst_ref=ret_v.at[at],
                send_sem=back_send.at[j], recv_sem=back_recv.at[j],
                device_id=device, device_id_type=MESH,
            ).start()

        @pl.loop(0, CHUNK // 8)
        def _(half):
            to_partners(j * (CHUNK // 8) + half, -1, give_back)

    recv_v[0] = send_v[0]
    serve(0, 1)
    ret_v[0] = res_v[0]

    @pl.loop(1, chunks)
    def _(j):
        serve(j, 0)

    def merge(q, first):
        waiter(ret_v, back_send, back_recv, 2 * q, first).wait_recv()
        waiter(ret_v, back_send, back_recv, 2 * q + 1, 0).wait_recv()
        share = merge_v[q]

        @pl.loop(0, width // tile)
        def _(n):
            cols = pl.ds(pl.multiple_of(n * tile, tile), tile)
            back = ret_v[pl.ds(2 * q * CHUNK, 2 * CHUNK), :, cols]
            back = back.astype(F32).reshape(2 * block, tile).astype(BF16)
            both = dot(share, back)
            shared_v[:, cols] += both[0:rows] + both[rows : 2 * rows]

    merge(0, 1)

    @pl.loop(1, chunks // 2)
    def _(q):
        merge(q, 0)

    @pl.loop(0, rows // 16)
    def _(b):
        at = pl.ds(pl.multiple_of(b * 16, 16), 16)
        out_ref[at, :] = layer_norm(shared_v[at, :], gout_ref[...]).astype(BF16)

    waiter(send_v, go_send, go_recv, 0, 1).wait_send()
    waiter(res_v, back_send, back_recv, 0, 1).wait_send()

    @pl.loop(1, chunks)
    def _(j):
        waiter(send_v, go_send, go_recv, j, 0).wait_send()
        waiter(res_v, back_send, back_recv, j, 0).wait_send()


def on_device(
    gate_pre, conv_in, conv_taps, recur_map, input_map, rate_logit, decay_shift, out_weight,
    residual, gain_mix, routes, route_weight, shared_gate, shared_up, shared_down,
    expert_gate, expert_up, expert_down, gain_out,
):
    tokens, channels = conv_in.shape
    rows, width = residual.shape
    heads, bw = recur_map.shape[:2]
    hidden = shared_gate.shape[1]
    groups, spans, peers, slots = channels // 128, tokens // SPAN, 2 * RING**3, 8
    any_spec = pl.BlockSpec(memory_space=pl.ANY)
    vmem_spec = pl.BlockSpec(memory_space=pltpu.VMEM)
    big = [
        gate_pre, conv_in, recur_map, input_map, out_weight, residual,
        shared_gate, shared_up, shared_down, expert_gate, expert_up, expert_down,
    ]
    small = [
        conv_taps, rate_logit.reshape(1, channels), decay_shift.T, gain_mix.reshape(1, width),
        gain_out.reshape(1, width), routes.T, route_weight.T,
    ]
    dma = pltpu.SemaphoreType.DMA
    chunks = peers // CHUNK
    return pl.pallas_call(
        layer_kernel,
        out_shape=jax.ShapeDtypeStruct((rows, width), BF16),
        in_specs=[any_spec] * (len(big) + len(small)),
        out_specs=vmem_spec,
        scratch_shapes=[pltpu.VMEM(v.shape, v.dtype) for v in small]
        + [
            pltpu.VMEM((tokens, 8), F32),
            pltpu.VMEM((tokens, channels), BF16),
            pltpu.VMEM((tokens, channels), BF16),
            pltpu.VMEM((heads, bw, bw), BF16),
            pltpu.VMEM((heads, bw, bw), BF16),
            pltpu.VMEM((2, channels, width), BF16),
            pltpu.VMEM((rows, width), BF16),
            pltpu.VMEM((width, hidden), BF16),
            pltpu.VMEM((width, hidden), BF16),
            pltpu.VMEM((hidden, width), BF16),
            pltpu.VMEM((width, hidden), BF16),
            pltpu.VMEM((width, hidden), BF16),
            pltpu.VMEM((hidden, width), BF16),
            pltpu.VMEM((HALO, channels), BF16),
            pltpu.VMEM((HALO + tokens, channels), F32),
            pltpu.VMEM((tokens, bw), F32),
            pltpu.VMEM((tokens, bw), F32),
            pltpu.VMEM((tokens, bw), BF16),
            pltpu.VMEM((groups, spans * PITCH, 128), F32),
            pltpu.VMEM((groups, spans * PITCH, 128), F32),
            pltpu.VMEM((groups, spans * PITCH, 128), F32),
            pltpu.VMEM((groups * spans, 128), F32),
            pltpu.VMEM((groups * spans, 128), F32),
            pltpu.VMEM((groups * spans, 128), F32),
            pltpu.VMEM((groups * spans, 128), F32),
            pltpu.VMEM((RING * RING, 2 * groups, 128), F32),
            pltpu.VMEM((RING, 2 * groups, 128), F32),
            pltpu.VMEM((tokens, channels), BF16),
            pltpu.VMEM((rows, channels), BF16),
            pltpu.VMEM((rows, width), F32),
            pltpu.VMEM((rows, width), BF16),
            pltpu.VMEM((rows, width), F32),
            pltpu.VMEM((CHUNK * slots, hidden), BF16),
            pltpu.VMEM((CHUNK * slots, width), BF16),
            pltpu.VMEM((peers * slots, rows), BF16),
            pltpu.VMEM((chunks // 2, 2 * rows, 2 * CHUNK * slots), BF16),
            pltpu.VMEM((peers, slots, width), BF16),
            pltpu.VMEM((peers, slots, width), BF16),
            pltpu.VMEM((peers, slots, width), BF16),
            pltpu.VMEM((peers, slots, width), BF16),
            dma((20,)), dma((2,)), dma((2,)), dma((2,)), dma((2,)),
            dma((chunks,)), dma((chunks,)), dma((chunks,)), dma((chunks,)),
        ],
        compiler_params=pltpu.CompilerParams(
            collective_id=0, has_side_effects=True, vmem_limit_bytes=52 * 1024 * 1024
        ),
        name="layer",
    )(*big, *small)


def solution(mesh):
    return jax.shard_map(
        on_device,
        mesh=mesh,
        in_specs=(
            P("sp", "tp"), P("sp", "tp"), P(None, "tp"), P("tp", None, None), P("tp", None, None),
            P("tp"), P("sp", "tp"), P(), P(("sp", "tp"), None), P(), P(("sp", "tp"), None),
            P(("sp", "tp"), None), P(), P(), P(), P(("sp", "tp"), None, None),
            P(("sp", "tp"), None, None), P(("sp", "tp"), None, None), P(),
        ),
        out_specs=P(("sp", "tp"), None),
        check_vma=False,
    )
```

```python
import functools

import jax
import jax.numpy as jnp
from jax import lax
from jax.experimental import pallas as pl
from jax.experimental.pallas import tpu as pltpu
from jax.sharding import PartitionSpec as P

ALPHA = 8.0**0.25
RATE_C = 8.0
NORM_EPS = 1e-05
MESH = pl.DeviceIdType.MESH
F32, BF16 = jnp.float32, jnp.bfloat16

RING = 4
CHUNK = 16
HALO = 16
SPAN = 32
PITCH = 40


def sigmoid(x):
    return 0.5 * jnp.tanh(0.5 * x) + 0.5


def silu(x):
    return x * sigmoid(x)


def minus_expm1(y):
    series = 1.0 + y * (1.0 / 7.0)
    for n in (6, 5, 4, 3, 2):
        series = 1.0 + (y * (1.0 / n)) * series
    return jnp.where(y > -0.5, -y * series, 1.0 - jnp.exp(y))


def gelu(x):
    inner = 0.7978845608028654 * (x + 0.044715 * (x * x * x))
    return 0.5 * x * (1.0 + jnp.tanh(inner))


def softplus(v):
    tail = jnp.exp(-jnp.abs(v))
    s = tail / (2.0 + tail)
    q = s * s
    series = 1.0 / 17.0
    for n in (15, 13, 11, 9, 7, 5, 3):
        series = 1.0 / n + q * series
    return jnp.maximum(v, 0.0) + 2.0 * s * (1.0 + q * series)


def dot(a, b):
    return jnp.dot(a, b, preferred_element_type=F32)


def layer_kernel(
    gate_hbm, conv_hbm, rmap_hbm, imap_hbm, outw_hbm, resid_hbm,
    sgate_hbm, sup_hbm, sdown_hbm, egate_hbm, eup_hbm, edown_hbm,
    taps_hbm, logit_hbm, shift_hbm, gmix_hbm, gout_hbm, routes_hbm, rw_hbm,
    out_ref,
    taps_ref, logit_ref, shift_t_ref, gmix_ref, gout_ref, routes_t_ref, rw_t_ref, shift_ref,
    gate_v, conv_v, rmap_v, imap_v, outw_v, resid_v,
    sgate_v, sup_v, sdown_v, egate_v, eup_v, edown_v,
    halo_v, ext_v, rpre_v, ipre_v, xb_v, a3, u3, g3,
    ca, ch, pa, ph, plane_buf, zbuf,
    mixed_v, theirs_v, proj_v, normed_v, shared_v, hid_v, rows_v,
    spread_v, merge_v, send_v, recv_v, res_v, ret_v,
    load_sem, halo_sem, line_send, line_recv, pair_sem,
    go_send, go_recv, back_send, back_recv,
):
    sp, tp = lax.axis_index("sp"), lax.axis_index("tp")
    x, y, z = sp % RING, (sp // RING) % RING, sp // (RING * RING)
    peers = RING * RING * RING * 2
    tokens, channels = conv_v.shape
    rows, width = normed_v.shape
    heads, bw = rmap_v.shape[0], rmap_v.shape[1]
    groups = channels // 128

    def wrap(v):
        return lax.rem(v, RING)

    def partners(m, sign):
        b, c = wrap(m), lax.div(m, RING)
        for a in range(RING):
            px = wrap(x + sign * a + RING)
            py = wrap(y + sign * (a + b) + 2 * RING)
            pz = wrap(z + sign * (a + c) + 2 * RING)
            for core in range(2):
                other = tp if core == 0 else 1 - tp
                yield a * 2 + core, {"sp": (pz * RING + py) * RING + px, "tp": other}

    def to_partners(m, sign, act):
        for n, device in partners(m, sign):
            if n == 0:

                @pl.when(m > 0)
                def _():
                    act(m * 8, device)

            else:
                act(m * 8 + n, device)

    def offset_of(i):
        core, k = i % 2, i // 2
        a, b, c = k % RING, (k // RING) % RING, k // (RING * RING)
        return core, a, (a + b) % RING, (a + c) % RING

    barrier = pltpu.get_barrier_semaphore()

    half = channels
    loads = [
        (conv_hbm, conv_v), (rmap_hbm, rmap_v), (imap_hbm, imap_v), (gate_hbm, gate_v),
        (outw_hbm.at[pl.ds(pl.multiple_of(tp * half, half), half)], outw_v.at[0]),
        (outw_hbm.at[pl.ds(pl.multiple_of((1 - tp) * half, half), half)], outw_v.at[1]),
        (resid_hbm, resid_v),
        (sgate_hbm, sgate_v), (sup_hbm, sup_v), (sdown_hbm, sdown_v),
        (egate_hbm.at[0], egate_v), (eup_hbm.at[0], eup_v), (edown_hbm.at[0], edown_v),
        (taps_hbm, taps_ref), (logit_hbm, logit_ref), (shift_hbm, shift_t_ref),
        (routes_hbm, routes_t_ref), (rw_hbm, rw_t_ref), (gmix_hbm, gmix_ref), (gout_hbm, gout_ref),
    ]
    loads = [pltpu.make_async_copy(s, d, load_sem.at[n]) for n, (s, d) in enumerate(loads)]
    for copy in loads[0:1] + loads[13:16] + loads[1:4] + loads[16:] + loads[4:5] + loads[6:7] + loads[5:6] + loads[7:13]:
        copy.start()

    @pl.loop(0, peers // 8)
    def _(m):
        def greet(at, device):
            pl.semaphore_signal(barrier, inc=1, device_id=device, device_id_type=MESH)

        to_partners(m, 1, greet)

    loads[0].wait()

    @pl.loop(0, tokens // 32)
    def _(b):
        at = pl.multiple_of(b * 32, 32)
        ext_v[pl.ds(HALO + at, 32), :] = conv_v[pl.ds(at, 32), :].astype(F32)

    for n in (13, 14, 15, 1, 2):
        loads[n].wait()
    rate = -RATE_C * softplus(-logit_ref[...])
    shift_rows = jnp.concatenate([shift_t_ref[...], jnp.zeros_like(shift_t_ref[...])], axis=0)
    shift_ref[...] = shift_rows.T

    def gates(h, first, count):
        cols = slice(h * bw, (h + 1) * bw)
        total = None
        for j in range(4):
            term = taps_ref[j : j + 1, cols].astype(F32) * ext_v[
                pl.ds(HALO + first - 3 + j, count), cols
            ]
            total = term if total is None else total + term
        conv_out = total.astype(BF16)
        xb_v[0:count, :] = conv_out
        rpre_v[0:count, :] = dot(conv_out, rmap_v[h])
        ipre_v[0:count, :] = dot(conv_out, imap_v[h])

        @pl.loop(0, count // SPAN)
        def _(b):
            at = pl.ds(pl.multiple_of(b * SPAN, SPAN), SPAN)
            r = sigmoid(rpre_v[at, :])
            i = sigmoid(ipre_v[at, :])
            shift = shift_ref[pl.ds(pl.multiple_of(first + b * SPAN, SPAN), SPAN), h : h + 1]
            log_decay = rate[:, cols] * r + shift
            a = jnp.exp(log_decay)
            u = jnp.sqrt(minus_expm1(2.0 * log_decay)) * i * xb_v[at, :].astype(F32)
            keep = pl.ds(pl.multiple_of((first // SPAN + b) * PITCH, 8), SPAN)
            for g in range(bw // 128):
                a3[h * (bw // 128) + g, keep, :] = a[:, g * 128 : (g + 1) * 128]
                u3[h * (bw // 128) + g, keep, :] = u[:, g * 128 : (g + 1) * 128]

    for h in range(heads // 2):
        gates(h, SPAN, tokens - SPAN)
    pl.semaphore_wait(barrier, peers - 1)
    halo = pltpu.make_async_remote_copy(
        src_ref=conv_v.at[pl.ds(tokens - HALO, HALO)], dst_ref=halo_v,
        send_sem=halo_sem.at[0], recv_sem=halo_sem.at[1],
        device_id={"sp": lax.rem(sp + 1, RING * RING * RING), "tp": tp}, device_id_type=MESH,
    )
    halo.start()
    for h in range(heads // 2, heads):
        gates(h, SPAN, tokens - SPAN)

    loads[3].wait()

    @pl.loop(0, tokens // SPAN)
    def _(b):
        at = pl.multiple_of(b * SPAN, SPAN)
        for g in range(groups):
            g3[g, pl.ds(pl.multiple_of(b * PITCH, 8), SPAN), :] = gelu(
                gate_v[pl.ds(at, SPAN), g * 128 : (g + 1) * 128].astype(F32)
            )

    halo.wait()
    ext_v[0:HALO, :] = jnp.where(sp == 0, 0.0, halo_v[...].astype(F32))
    for h in range(heads):
        gates(h, 0, SPAN)

    spans = tokens // SPAN

    def walk(s, carry):
        out = []
        for g in range(groups):
            at = pl.ds(s, spans, stride=PITCH)
            a, u = a3[g, at, :], u3[g, at, :]
            out.append((carry[g][0] * a, a * carry[g][1] + u))
        return tuple(out)

    one, nought = jnp.ones((spans, 128), F32), jnp.zeros((spans, 128), F32)
    ends = lax.fori_loop(0, SPAN, walk, tuple((one, nought) for _ in range(groups)), unroll=4)
    for g in range(groups):
        ca[g * spans : (g + 1) * spans, :] = ends[g][0]
        ch[g * spans : (g + 1) * spans, :] = ends[g][1]
    run_a, run_h = jnp.ones((groups, 128), F32), jnp.zeros((groups, 128), F32)
    for c in range(spans):
        at = pl.ds(c, groups, stride=spans)
        pa[at, :], ph[at, :] = run_a, run_h
        a, h = ca[at, :], ch[at, :]
        run_a, run_h = run_a * a, a * run_h + h

    def exchange(n, buf, here, stride, whole_a, whole_h):
        count = buf.shape[0]
        buf[here, 0:groups, :] = whole_a
        buf[here, groups : 2 * groups, :] = whole_h

        @pl.loop(1, count)
        def _(d):
            pltpu.make_async_remote_copy(
                src_ref=buf.at[here], dst_ref=buf.at[here],
                send_sem=line_send.at[n], recv_sem=line_recv.at[n],
                device_id={"sp": sp + (lax.rem(here + d, count) - here) * stride, "tp": tp},
                device_id_type=MESH,
            ).start()

    def arrived(n, buf):
        others = buf.at[pl.ds(0, buf.shape[0] - 1)]
        copy = pltpu.make_async_remote_copy(
            src_ref=others, dst_ref=others, send_sem=line_send.at[n], recv_sem=line_recv.at[n],
            device_id={"sp": sp, "tp": 1 - tp}, device_id_type=MESH,
        )
        copy.wait_recv()
        copy.wait_send()

    in_plane = y * RING + x
    exchange(0, plane_buf, in_plane, 1, run_a, run_h)

    loads[16].wait()
    loads[17].wait()
    slots = 8
    sub_e = lax.broadcasted_iota(jnp.int32, (peers, rows), 0)
    member_t, weight_t = jnp.zeros((peers, rows), F32), jnp.zeros((peers, rows), F32)
    for k in range(4):
        hit = routes_t_ref[k : k + 1, :] == sub_e
        member_t = member_t + jnp.where(hit, 1.0, 0.0)
        weight_t = weight_t + jnp.where(hit, rw_t_ref[k : k + 1, :], 0.0)
    i0 = lax.broadcasted_iota(jnp.int32, (rows, rows), 0)
    i1 = lax.broadcasted_iota(jnp.int32, (rows, rows), 1)
    above = jnp.where(i0 < i1, 1.0, 0.0).astype(BF16)
    ranks_t = (dot(member_t.astype(BF16), above) + 1.0) * member_t
    place_t = ranks_t.astype(BF16)
    place = ranks_t.T.astype(BF16)
    weight = weight_t.T
    weight_hi = weight.astype(BF16)
    weight_lo = (weight - weight_hi.astype(F32)).astype(BF16)

    def expert_of(i):
        core, dx, dy, dz = offset_of(i)
        chip = (((z + dz) % RING) * RING + (y + dy) % RING) * RING + (x + dx) % RING
        return chip * 2 + (tp + core) % 2

    wide = 256
    slot = (lax.broadcasted_iota(jnp.int32, (wide, rows), 0) % slots + 1).astype(F32)
    slot_t = (lax.broadcasted_iota(jnp.int32, (rows, wide), 1) % slots + 1).astype(F32)
    step_i = lax.broadcasted_iota(jnp.int32, (wide, 1), 0)
    step_t = lax.broadcasted_iota(jnp.int32, (1, wide), 1)
    name_i = lax.broadcasted_iota(jnp.int32, (wide, peers), 1)
    name_t = lax.broadcasted_iota(jnp.int32, (peers, wide), 0)
    for q in range(peers * slots // wide):
        pick = jnp.where(expert_of((step_i + q * wide) // slots) == name_i, 1.0, 0.0).astype(BF16)
        found = dot(pick, place_t)
        spread_v[q * wide : (q + 1) * wide, :] = jnp.where(found == slot, 1.0, 0.0).astype(BF16)

    arrived(0, plane_buf)
    plane_a, plane_h = plane_buf[0, 0:groups, :], plane_buf[0, groups : 2 * groups, :]
    for n in range(1, RING * RING):
        a, h = plane_buf[n, 0:groups, :], plane_buf[n, groups : 2 * groups, :]
        plane_a, plane_h = plane_a * a, plane_h * a + h
    exchange(1, zbuf, z, RING * RING, plane_a, plane_h)
    for q in range(peers * slots // wide):
        pick_t = jnp.where(expert_of((step_t + q * wide) // slots) == name_t, 1.0, 0.0).astype(BF16)
        match = dot(place, pick_t) == slot_t
        merge_v[q, 0:rows, :] = jnp.where(match, dot(weight_hi, pick_t), 0.0).astype(BF16)
        merge_v[q, rows : 2 * rows, :] = jnp.where(match, dot(weight_lo, pick_t), 0.0).astype(BF16)

    arrived(1, zbuf)

    state = jnp.zeros((groups, 128), F32)
    for buf, here in ((zbuf, z), (plane_buf, in_plane)):
        for n in range(buf.shape[0] - 1):
            a, h = buf[n, 0:groups, :], buf[n, groups : 2 * groups, :]
            state = jnp.where(n < here, a * state + h, state)

    starts = tuple(
        pa[g * spans : (g + 1) * spans, :] * state[g : g + 1, :] + ph[g * spans : (g + 1) * spans, :]
        for g in range(groups)
    )

    def rewalk(s, carry):
        out = []
        for g in range(groups):
            at = pl.ds(s, spans, stride=PITCH)
            h = a3[g, at, :] * carry[g] + u3[g, at, :]
            u3[g, at, :] = h * g3[g, at, :]
            out.append(h)
        return tuple(out)

    lax.fori_loop(0, SPAN, rewalk, starts, unroll=4)

    def round_rows(first):
        @pl.loop(0, rows // SPAN)
        def _(b):
            at = pl.ds(pl.multiple_of(first + b * SPAN, SPAN), SPAN)
            keep = pl.ds(pl.multiple_of((first // SPAN + b) * PITCH, 8), SPAN)
            for g in range(groups):
                mixed_v[at, g * 128 : (g + 1) * 128] = u3[g, keep, :].astype(BF16)

    round_rows((1 - tp) * rows)
    pair = pltpu.make_async_remote_copy(
        src_ref=mixed_v.at[pl.ds(pl.multiple_of((1 - tp) * rows, rows), rows)], dst_ref=theirs_v,
        send_sem=pair_sem.at[0], recv_sem=pair_sem.at[1],
        device_id={"sp": sp, "tp": 1 - tp}, device_id_type=MESH,
    )
    pair.start()
    round_rows(tp * rows)

    tile = 256
    mine = mixed_v[pl.ds(pl.multiple_of(tp * rows, rows), rows), :]
    loads[4].wait()
    loads[6].wait()

    @pl.loop(0, width // tile)
    def _(n):
        cols = pl.ds(pl.multiple_of(n * tile, tile), tile)
        proj_v[:, cols] = ALPHA * resid_v[:, cols].astype(F32) + dot(mine, outw_v[0, :, cols])

    loads[5].wait()
    pair.wait()
    theirs = theirs_v[...]

    @pl.loop(0, width // tile)
    def _(n):
        cols = pl.ds(pl.multiple_of(n * tile, tile), tile)
        proj_v[:, cols] += dot(theirs, outw_v[1, :, cols])

    def layer_norm(values, gains):
        center = values - jnp.mean(values, axis=-1, keepdims=True)
        spread = jnp.mean(center * center, axis=-1, keepdims=True)
        return center * lax.rsqrt(spread + NORM_EPS) * gains

    loads[18].wait()
    loads[19].wait()

    @pl.loop(0, rows // 16, unroll=4)
    def _(b):
        at = pl.ds(pl.multiple_of(b * 16, 16), 16)
        normed_v[at, :] = layer_norm(proj_v[at, :], gmix_ref[...]).astype(BF16)

    chunks = peers // CHUNK
    block = CHUNK * slots

    def chunk_of(ref, j):
        return ref.at[pl.ds(pl.multiple_of(j * CHUNK, CHUNK), CHUNK)]

    @pl.loop(0, chunks)
    def _(j):
        pick = spread_v[pl.ds(pl.multiple_of(j * block, block), block), :]
        for n in range(width // 512):
            part = dot(pick, normed_v[:, n * 512 : (n + 1) * 512])
            send_v[pl.ds(j * CHUNK, CHUNK), :, n * 512 : (n + 1) * 512] = part.reshape(
                CHUNK, slots, 512
            ).astype(BF16)

        def give(at, device):
            pltpu.make_async_remote_copy(
                src_ref=send_v.at[at], dst_ref=recv_v.at[at],
                send_sem=go_send.at[j], recv_sem=go_recv.at[j],
                device_id=device, device_id_type=MESH,
            ).start()

        @pl.loop(0, CHUNK // 8)
        def _(half):
            to_partners(j * (CHUNK // 8) + half, 1, give)

    def expert(x_in, gate, up, down, store):
        @pl.loop(0, gate.shape[1] // tile)
        def _(n):
            cols = pl.ds(pl.multiple_of(n * tile, tile), tile)
            hid_v[:, cols] = (silu(dot(x_in, gate[:, cols])) * dot(x_in, up[:, cols])).astype(BF16)

        hidden = hid_v[...]

        @pl.loop(0, width // tile)
        def _(n):
            cols = pl.ds(pl.multiple_of(n * tile, tile), tile)
            store(cols, dot(hidden, down[:, cols]))

    def keep_shared(cols, value):
        shared_v[:, cols] = ALPHA * normed_v[:, cols].astype(F32) + value

    loads[7].wait()
    loads[8].wait()
    loads[9].wait()
    expert(normed_v[...], sgate_v, sup_v, sdown_v, keep_shared)
    loads[10].wait()
    loads[11].wait()
    loads[12].wait()

    def waiter(ref, send, recv, j, first):
        part = ref.at[pl.ds(pl.multiple_of(j * CHUNK, CHUNK) + first, CHUNK - first)]
        return pltpu.make_async_remote_copy(
            src_ref=part, dst_ref=part, send_sem=send.at[j], recv_sem=recv.at[j],
            device_id={"sp": sp, "tp": 1 - tp}, device_id_type=MESH,
        )

    def serve(j, first):
        waiter(recv_v, go_send, go_recv, j, first).wait_recv()
        chosen = recv_v[pl.ds(j * CHUNK, CHUNK)]
        rows_v[...] = chosen.astype(F32).reshape(block, width).astype(BF16)

        def give(cols, value):
            res_v[pl.ds(j * CHUNK, CHUNK), :, cols] = value.reshape(CHUNK, slots, tile).astype(BF16)

        expert(rows_v[...], egate_v, eup_v, edown_v, give)

        def give_back(at, device):
            pltpu.make_async_remote_copy(
                src_ref=res_v.at[at], dst_ref=ret_v.at[at],
                send_sem=back_send.at[j], recv_sem=back_recv.at[j],
                device_id=device, device_id_type=MESH,
            ).start()

        @pl.loop(0, CHUNK // 8)
        def _(half):
            to_partners(j * (CHUNK // 8) + half, -1, give_back)

    recv_v[0] = send_v[0]
    serve(0, 1)
    ret_v[0] = res_v[0]

    @pl.loop(1, chunks)
    def _(j):
        serve(j, 0)

    def merge(q, first):
        waiter(ret_v, back_send, back_recv, 2 * q, first).wait_recv()
        waiter(ret_v, back_send, back_recv, 2 * q + 1, 0).wait_recv()
        share = merge_v[q]

        @pl.loop(0, width // tile)
        def _(n):
            cols = pl.ds(pl.multiple_of(n * tile, tile), tile)
            back = ret_v[pl.ds(2 * q * CHUNK, 2 * CHUNK), :, cols]
            back = back.astype(F32).reshape(2 * block, tile).astype(BF16)
            both = dot(share, back)
            shared_v[:, cols] += both[0:rows] + both[rows : 2 * rows]

    merge(0, 1)

    @pl.loop(1, chunks // 2)
    def _(q):
        merge(q, 0)

    @pl.loop(0, rows // 16, unroll=4)
    def _(b):
        at = pl.ds(pl.multiple_of(b * 16, 16), 16)
        out_ref[at, :] = layer_norm(shared_v[at, :], gout_ref[...]).astype(BF16)

    waiter(send_v, go_send, go_recv, 0, 1).wait_send()
    waiter(res_v, back_send, back_recv, 0, 1).wait_send()

    @pl.loop(1, chunks)
    def _(j):
        waiter(send_v, go_send, go_recv, j, 0).wait_send()
        waiter(res_v, back_send, back_recv, j, 0).wait_send()


def on_device(
    gate_pre, conv_in, conv_taps, recur_map, input_map, rate_logit, decay_shift, out_weight,
    residual, gain_mix, routes, route_weight, shared_gate, shared_up, shared_down,
    expert_gate, expert_up, expert_down, gain_out,
):
    tokens, channels = conv_in.shape
    rows, width = residual.shape
    heads, bw = recur_map.shape[:2]
    hidden = shared_gate.shape[1]
    groups, spans, peers, slots = channels // 128, tokens // SPAN, 2 * RING**3, 8
    any_spec = pl.BlockSpec(memory_space=pl.ANY)
    vmem_spec = pl.BlockSpec(memory_space=pltpu.VMEM)
    big = [
        gate_pre, conv_in, recur_map, input_map, out_weight, residual,
        shared_gate, shared_up, shared_down, expert_gate, expert_up, expert_down,
    ]
    small = [
        conv_taps, rate_logit.reshape(1, channels), decay_shift.T, gain_mix.reshape(1, width),
        gain_out.reshape(1, width), routes.T, route_weight.T,
    ]
    dma = pltpu.SemaphoreType.DMA
    chunks = peers // CHUNK
    return pl.pallas_call(
        layer_kernel,
        out_shape=jax.ShapeDtypeStruct((rows, width), BF16),
        in_specs=[any_spec] * (len(big) + len(small)),
        out_specs=vmem_spec,
        scratch_shapes=[pltpu.VMEM(v.shape, v.dtype) for v in small]
        + [
            pltpu.VMEM((tokens, 8), F32),
            pltpu.VMEM((tokens, channels), BF16),
            pltpu.VMEM((tokens, channels), BF16),
            pltpu.VMEM((heads, bw, bw), BF16),
            pltpu.VMEM((heads, bw, bw), BF16),
            pltpu.VMEM((2, channels, width), BF16),
            pltpu.VMEM((rows, width), BF16),
            pltpu.VMEM((width, hidden), BF16),
            pltpu.VMEM((width, hidden), BF16),
            pltpu.VMEM((hidden, width), BF16),
            pltpu.VMEM((width, hidden), BF16),
            pltpu.VMEM((width, hidden), BF16),
            pltpu.VMEM((hidden, width), BF16),
            pltpu.VMEM((HALO, channels), BF16),
            pltpu.VMEM((HALO + tokens, channels), F32),
            pltpu.VMEM((tokens, bw), F32),
            pltpu.VMEM((tokens, bw), F32),
            pltpu.VMEM((tokens, bw), BF16),
            pltpu.VMEM((groups, spans * PITCH, 128), F32),
            pltpu.VMEM((groups, spans * PITCH, 128), F32),
            pltpu.VMEM((groups, spans * PITCH, 128), F32),
            pltpu.VMEM((groups * spans, 128), F32),
            pltpu.VMEM((groups * spans, 128), F32),
            pltpu.VMEM((groups * spans, 128), F32),
            pltpu.VMEM((groups * spans, 128), F32),
            pltpu.VMEM((RING * RING, 2 * groups, 128), F32),
            pltpu.VMEM((RING, 2 * groups, 128), F32),
            pltpu.VMEM((tokens, channels), BF16),
            pltpu.VMEM((rows, channels), BF16),
            pltpu.VMEM((rows, width), F32),
            pltpu.VMEM((rows, width), BF16),
            pltpu.VMEM((rows, width), F32),
            pltpu.VMEM((CHUNK * slots, hidden), BF16),
            pltpu.VMEM((CHUNK * slots, width), BF16),
            pltpu.VMEM((peers * slots, rows), BF16),
            pltpu.VMEM((chunks // 2, 2 * rows, 2 * CHUNK * slots), BF16),
            pltpu.VMEM((peers, slots, width), BF16),
            pltpu.VMEM((peers, slots, width), BF16),
            pltpu.VMEM((peers, slots, width), BF16),
            pltpu.VMEM((peers, slots, width), BF16),
            dma((20,)), dma((2,)), dma((2,)), dma((2,)), dma((2,)),
            dma((chunks,)), dma((chunks,)), dma((chunks,)), dma((chunks,)),
        ],
        compiler_params=pltpu.CompilerParams(
            collective_id=0, has_side_effects=True, vmem_limit_bytes=52 * 1024 * 1024
        ),
        name="layer",
    )(*(pltpu.with_memory_space_constraint(v, pltpu.HBM) for v in (*big, *small)))


def solution(mesh):
    return jax.shard_map(
        on_device,
        mesh=mesh,
        in_specs=(
            P("sp", "tp"), P("sp", "tp"), P(None, "tp"), P("tp", None, None), P("tp", None, None),
            P("tp"), P("sp", "tp"), P(), P(("sp", "tp"), None), P(), P(("sp", "tp"), None),
            P(("sp", "tp"), None), P(), P(), P(), P(("sp", "tp"), None, None),
            P(("sp", "tp"), None, None), P(("sp", "tp"), None, None), P(),
        ),
        out_specs=P(("sp", "tp"), None),
        check_vma=False,
    )
```

```python
import functools

import jax
import jax.numpy as jnp
from jax import lax
from jax.experimental import pallas as pl
from jax.experimental.pallas import tpu as pltpu
from jax.sharding import PartitionSpec as P

ALPHA = 8.0**0.25
RATE_C = 8.0
NORM_EPS = 1e-05
MESH = pl.DeviceIdType.MESH
F32, BF16 = jnp.float32, jnp.bfloat16

RING = 4
CHUNK = 16
HALO = 16
SPAN = 32
PITCH = 40


def sigmoid(x):
    return 0.5 * jnp.tanh(0.5 * x) + 0.5


def silu(x):
    return x * sigmoid(x)


def minus_expm1(y):
    series = 1.0 + y * (1.0 / 7.0)
    for n in (6, 5, 4, 3, 2):
        series = 1.0 + (y * (1.0 / n)) * series
    return jnp.where(y > -0.5, -y * series, 1.0 - jnp.exp(y))


def gelu(x):
    inner = 0.7978845608028654 * (x + 0.044715 * (x * x * x))
    return 0.5 * x * (1.0 + jnp.tanh(inner))


def softplus(v):
    tail = jnp.exp(-jnp.abs(v))
    s = tail / (2.0 + tail)
    q = s * s
    series = 1.0 / 17.0
    for n in (15, 13, 11, 9, 7, 5, 3):
        series = 1.0 / n + q * series
    return jnp.maximum(v, 0.0) + 2.0 * s * (1.0 + q * series)


def dot(a, b):
    return jnp.dot(a, b, preferred_element_type=F32)


def layer_kernel(
    gate_hbm, conv_hbm, rmap_hbm, imap_hbm, outw_hbm, resid_hbm,
    sgate_hbm, sup_hbm, sdown_hbm, egate_hbm, eup_hbm, edown_hbm,
    taps_hbm, logit_hbm, shift_hbm, gmix_hbm, gout_hbm, routes_hbm, rw_hbm,
    out_ref,
    taps_ref, logit_ref, shift_t_ref, gmix_ref, gout_ref, routes_t_ref, rw_t_ref, shift_ref,
    gate_v, conv_v, rmap_v, imap_v, outw_v, resid_v,
    sgate_v, sup_v, sdown_v, egate_v, eup_v, edown_v,
    halo_v, ext_v, rpre_v, ipre_v, xb_v, a3, u3, g3,
    ca, ch, pa, ph, plane_buf, zbuf,
    mixed_v, theirs_v, proj_v, normed_v, shared_v, hid_v, rows_v,
    spread_v, merge_v, send_v, recv_v, res_v, ret_v,
    load_sem, halo_sem, line_send, line_recv, pair_sem,
    go_send, go_recv, back_send, back_recv,
):
    sp, tp = lax.axis_index("sp"), lax.axis_index("tp")
    x, y, z = sp % RING, (sp // RING) % RING, sp // (RING * RING)
    peers = RING * RING * RING * 2
    tokens, channels = conv_v.shape
    rows, width = normed_v.shape
    heads, bw = rmap_v.shape[0], rmap_v.shape[1]
    groups = channels // 128

    def wrap(v):
        return lax.rem(v, RING)

    turn = 1 - 2 * tp

    def partners(m, signs):
        b, c = wrap(m), lax.div(m, RING)
        for a in range(RING):
            for core, sign in enumerate(signs):
                px = wrap(x + sign * a + RING)
                py = wrap(y + sign * (a + b) + 2 * RING)
                pz = wrap(z + sign * (a + c) + 2 * RING)
                other = tp if core == 0 else 1 - tp
                yield a * 2 + core, {"sp": (pz * RING + py) * RING + px, "tp": other}

    ahead, behind = (turn, turn), (-turn, turn)

    def to_partners(m, signs, act):
        for n, device in partners(m, signs):
            if n == 0:

                @pl.when(m > 0)
                def _():
                    act(m * 8, device)

            else:
                act(m * 8 + n, device)

    def offset_of(i):
        core, k = i % 2, i // 2
        a, b, c = k % RING, (k // RING) % RING, k // (RING * RING)
        return core, a, (a + b) % RING, (a + c) % RING

    barrier = pltpu.get_barrier_semaphore()

    half = channels
    loads = [
        (conv_hbm, conv_v), (rmap_hbm, rmap_v), (imap_hbm, imap_v), (gate_hbm, gate_v),
        (outw_hbm.at[pl.ds(pl.multiple_of(tp * half, half), half)], outw_v.at[0]),
        (outw_hbm.at[pl.ds(pl.multiple_of((1 - tp) * half, half), half)], outw_v.at[1]),
        (resid_hbm, resid_v),
        (sgate_hbm, sgate_v), (sup_hbm, sup_v), (sdown_hbm, sdown_v),
        (egate_hbm.at[0], egate_v), (eup_hbm.at[0], eup_v), (edown_hbm.at[0], edown_v),
        (taps_hbm, taps_ref), (logit_hbm, logit_ref), (shift_hbm, shift_t_ref),
        (routes_hbm, routes_t_ref), (rw_hbm, rw_t_ref), (gmix_hbm, gmix_ref), (gout_hbm, gout_ref),
    ]
    loads = [pltpu.make_async_copy(s, d, load_sem.at[n]) for n, (s, d) in enumerate(loads)]
    @pl.loop(0, peers // 8)
    def _(m):
        def greet(at, device):
            pl.semaphore_signal(barrier, inc=1, device_id=device, device_id_type=MESH)

        to_partners(m, ahead, greet)

    for copy in loads[0:1] + loads[13:16] + loads[1:4] + loads[16:] + loads[4:5] + loads[6:7] + loads[5:6] + loads[7:13]:
        copy.start()

    loads[0].wait()

    @pl.loop(0, tokens // 32)
    def _(b):
        at = pl.multiple_of(b * 32, 32)
        ext_v[pl.ds(HALO + at, 32), :] = conv_v[pl.ds(at, 32), :].astype(F32)

    for n in (13, 14, 15, 1, 2):
        loads[n].wait()
    rate = -RATE_C * softplus(-logit_ref[...])
    shift_rows = jnp.concatenate([shift_t_ref[...], jnp.zeros_like(shift_t_ref[...])], axis=0)
    shift_ref[...] = shift_rows.T

    def gates(h, first, count):
        cols = slice(h * bw, (h + 1) * bw)
        total = None
        for j in range(4):
            term = taps_ref[j : j + 1, cols].astype(F32) * ext_v[
                pl.ds(HALO + first - 3 + j, count), cols
            ]
            total = term if total is None else total + term
        conv_out = total.astype(BF16)
        xb_v[0:count, :] = conv_out
        rpre_v[0:count, :] = dot(conv_out, rmap_v[h])
        ipre_v[0:count, :] = dot(conv_out, imap_v[h])

        @pl.loop(0, count // SPAN)
        def _(b):
            at = pl.ds(pl.multiple_of(b * SPAN, SPAN), SPAN)
            r = sigmoid(rpre_v[at, :])
            i = sigmoid(ipre_v[at, :])
            shift = shift_ref[pl.ds(pl.multiple_of(first + b * SPAN, SPAN), SPAN), h : h + 1]
            log_decay = rate[:, cols] * r + shift
            a = jnp.exp(log_decay)
            u = jnp.sqrt(minus_expm1(2.0 * log_decay)) * i * xb_v[at, :].astype(F32)
            keep = pl.ds(pl.multiple_of((first // SPAN + b) * PITCH, 8), SPAN)
            for g in range(bw // 128):
                a3[h * (bw // 128) + g, keep, :] = a[:, g * 128 : (g + 1) * 128]
                u3[h * (bw // 128) + g, keep, :] = u[:, g * 128 : (g + 1) * 128]

    for h in range(heads // 2):
        gates(h, SPAN, tokens - SPAN)
    pl.semaphore_wait(barrier, peers - 1)
    halo = pltpu.make_async_remote_copy(
        src_ref=conv_v.at[pl.ds(tokens - HALO, HALO)], dst_ref=halo_v,
        send_sem=halo_sem.at[0], recv_sem=halo_sem.at[1],
        device_id={"sp": lax.rem(sp + 1, RING * RING * RING), "tp": tp}, device_id_type=MESH,
    )
    halo.start()
    for h in range(heads // 2, heads):
        gates(h, SPAN, tokens - SPAN)

    loads[3].wait()

    @pl.loop(0, tokens // SPAN)
    def _(b):
        at = pl.multiple_of(b * SPAN, SPAN)
        for g in range(groups):
            g3[g, pl.ds(pl.multiple_of(b * PITCH, 8), SPAN), :] = gelu(
                gate_v[pl.ds(at, SPAN), g * 128 : (g + 1) * 128].astype(F32)
            )

    halo.wait()
    ext_v[0:HALO, :] = jnp.where(sp == 0, 0.0, halo_v[...].astype(F32))
    for h in range(heads):
        gates(h, 0, SPAN)

    spans = tokens // SPAN

    def walk(s, carry):
        out = []
        for g in range(groups):
            at = pl.ds(s, spans, stride=PITCH)
            a, u = a3[g, at, :], u3[g, at, :]
            out.append((carry[g][0] * a, a * carry[g][1] + u))
        return tuple(out)

    one, nought = jnp.ones((spans, 128), F32), jnp.zeros((spans, 128), F32)
    ends = lax.fori_loop(0, SPAN, walk, tuple((one, nought) for _ in range(groups)), unroll=4)
    for g in range(groups):
        ca[g * spans : (g + 1) * spans, :] = ends[g][0]
        ch[g * spans : (g + 1) * spans, :] = ends[g][1]
    run_a, run_h = jnp.ones((groups, 128), F32), jnp.zeros((groups, 128), F32)
    for c in range(spans):
        at = pl.ds(c, groups, stride=spans)
        pa[at, :], ph[at, :] = run_a, run_h
        a, h = ca[at, :], ch[at, :]
        run_a, run_h = run_a * a, a * run_h + h

    def exchange(n, buf, here, stride, whole_a, whole_h):
        count = buf.shape[0]
        buf[here, 0:groups, :] = whole_a
        buf[here, groups : 2 * groups, :] = whole_h

        @pl.loop(1, count)
        def _(d):
            pltpu.make_async_remote_copy(
                src_ref=buf.at[here], dst_ref=buf.at[here],
                send_sem=line_send.at[n], recv_sem=line_recv.at[n],
                device_id={"sp": sp + (lax.rem(here + d, count) - here) * stride, "tp": tp},
                device_id_type=MESH,
            ).start()

    def arrived(n, buf):
        others = buf.at[pl.ds(0, buf.shape[0] - 1)]
        copy = pltpu.make_async_remote_copy(
            src_ref=others, dst_ref=others, send_sem=line_send.at[n], recv_sem=line_recv.at[n],
            device_id={"sp": sp, "tp": 1 - tp}, device_id_type=MESH,
        )
        copy.wait_recv()
        copy.wait_send()

    in_plane = y * RING + x
    exchange(0, plane_buf, in_plane, 1, run_a, run_h)

    loads[16].wait()
    loads[17].wait()
    slots = 8
    sub_e = lax.broadcasted_iota(jnp.int32, (peers, rows), 0)
    member_t, weight_t = jnp.zeros((peers, rows), F32), jnp.zeros((peers, rows), F32)
    for k in range(4):
        hit = routes_t_ref[k : k + 1, :] == sub_e
        member_t = member_t + jnp.where(hit, 1.0, 0.0)
        weight_t = weight_t + jnp.where(hit, rw_t_ref[k : k + 1, :], 0.0)
    i0 = lax.broadcasted_iota(jnp.int32, (rows, rows), 0)
    i1 = lax.broadcasted_iota(jnp.int32, (rows, rows), 1)
    above = jnp.where(i0 < i1, 1.0, 0.0).astype(BF16)
    ranks_t = (dot(member_t.astype(BF16), above) + 1.0) * member_t
    place_t = ranks_t.astype(BF16)
    place = ranks_t.T.astype(BF16)
    weight = weight_t.T
    weight_hi = weight.astype(BF16)
    weight_lo = (weight - weight_hi.astype(F32)).astype(BF16)

    def expert_of(i):
        core, dx, dy, dz = offset_of(i)
        chip = ((z + turn * dz + RING) % RING) * RING + (y + turn * dy + RING) % RING
        chip = chip * RING + (x + turn * dx + RING) % RING
        return chip * 2 + (tp + core) % 2

    wide = 256
    slot = (lax.broadcasted_iota(jnp.int32, (wide, rows), 0) % slots + 1).astype(F32)
    slot_t = (lax.broadcasted_iota(jnp.int32, (rows, wide), 1) % slots + 1).astype(F32)
    step_i = lax.broadcasted_iota(jnp.int32, (wide, 1), 0)
    step_t = lax.broadcasted_iota(jnp.int32, (1, wide), 1)
    name_i = lax.broadcasted_iota(jnp.int32, (wide, peers), 1)
    name_t = lax.broadcasted_iota(jnp.int32, (peers, wide), 0)
    for q in range(peers * slots // wide):
        pick = jnp.where(expert_of((step_i + q * wide) // slots) == name_i, 1.0, 0.0).astype(BF16)
        found = dot(pick, place_t)
        spread_v[q * wide : (q + 1) * wide, :] = jnp.where(found == slot, 1.0, 0.0).astype(BF16)

    arrived(0, plane_buf)
    plane_a, plane_h = plane_buf[0, 0:groups, :], plane_buf[0, groups : 2 * groups, :]
    for n in range(1, RING * RING):
        a, h = plane_buf[n, 0:groups, :], plane_buf[n, groups : 2 * groups, :]
        plane_a, plane_h = plane_a * a, plane_h * a + h
    exchange(1, zbuf, z, RING * RING, plane_a, plane_h)
    for q in range(peers * slots // wide):
        pick_t = jnp.where(expert_of((step_t + q * wide) // slots) == name_t, 1.0, 0.0).astype(BF16)
        match = dot(place, pick_t) == slot_t
        merge_v[q, 0:rows, :] = jnp.where(match, dot(weight_hi, pick_t), 0.0).astype(BF16)
        merge_v[q, rows : 2 * rows, :] = jnp.where(match, dot(weight_lo, pick_t), 0.0).astype(BF16)

    arrived(1, zbuf)

    state = jnp.zeros((groups, 128), F32)
    for buf, here in ((zbuf, z), (plane_buf, in_plane)):
        for n in range(buf.shape[0] - 1):
            a, h = buf[n, 0:groups, :], buf[n, groups : 2 * groups, :]
            state = jnp.where(n < here, a * state + h, state)

    starts = tuple(
        pa[g * spans : (g + 1) * spans, :] * state[g : g + 1, :] + ph[g * spans : (g + 1) * spans, :]
        for g in range(groups)
    )

    def rewalk(s, carry):
        out = []
        for g in range(groups):
            at = pl.ds(s, spans, stride=PITCH)
            h = a3[g, at, :] * carry[g] + u3[g, at, :]
            u3[g, at, :] = h * g3[g, at, :]
            out.append(h)
        return tuple(out)

    lax.fori_loop(0, SPAN, rewalk, starts, unroll=4)

    def round_rows(first):
        @pl.loop(0, rows // SPAN)
        def _(b):
            at = pl.ds(pl.multiple_of(first + b * SPAN, SPAN), SPAN)
            keep = pl.ds(pl.multiple_of((first // SPAN + b) * PITCH, 8), SPAN)
            for g in range(groups):
                mixed_v[at, g * 128 : (g + 1) * 128] = u3[g, keep, :].astype(BF16)

    round_rows((1 - tp) * rows)
    pair = pltpu.make_async_remote_copy(
        src_ref=mixed_v.at[pl.ds(pl.multiple_of((1 - tp) * rows, rows), rows)], dst_ref=theirs_v,
        send_sem=pair_sem.at[0], recv_sem=pair_sem.at[1],
        device_id={"sp": sp, "tp": 1 - tp}, device_id_type=MESH,
    )
    pair.start()
    round_rows(tp * rows)

    tile = 256
    mine = mixed_v[pl.ds(pl.multiple_of(tp * rows, rows), rows), :]
    loads[4].wait()
    loads[6].wait()

    @pl.loop(0, width // tile)
    def _(n):
        cols = pl.ds(pl.multiple_of(n * tile, tile), tile)
        proj_v[:, cols] = ALPHA * resid_v[:, cols].astype(F32) + dot(mine, outw_v[0, :, cols])

    loads[5].wait()
    pair.wait()
    theirs = theirs_v[...]

    @pl.loop(0, width // tile)
    def _(n):
        cols = pl.ds(pl.multiple_of(n * tile, tile), tile)
        proj_v[:, cols] += dot(theirs, outw_v[1, :, cols])

    def layer_norm(values, gains):
        center = values - jnp.mean(values, axis=-1, keepdims=True)
        spread = jnp.mean(center * center, axis=-1, keepdims=True)
        return center * lax.rsqrt(spread + NORM_EPS) * gains

    loads[18].wait()
    loads[19].wait()

    @pl.loop(0, rows // 16, unroll=4)
    def _(b):
        at = pl.ds(pl.multiple_of(b * 16, 16), 16)
        normed_v[at, :] = layer_norm(proj_v[at, :], gmix_ref[...]).astype(BF16)

    chunks = peers // CHUNK
    block = CHUNK * slots

    def chunk_of(ref, j):
        return ref.at[pl.ds(pl.multiple_of(j * CHUNK, CHUNK), CHUNK)]

    @pl.loop(0, chunks)
    def _(j):
        pick = spread_v[pl.ds(pl.multiple_of(j * block, block), block), :]
        for n in range(width // 512):
            part = dot(pick, normed_v[:, n * 512 : (n + 1) * 512])
            send_v[pl.ds(j * CHUNK, CHUNK), :, n * 512 : (n + 1) * 512] = part.reshape(
                CHUNK, slots, 512
            ).astype(BF16)

        def give(at, device):
            pltpu.make_async_remote_copy(
                src_ref=send_v.at[at], dst_ref=recv_v.at[at],
                send_sem=go_send.at[j], recv_sem=go_recv.at[j],
                device_id=device, device_id_type=MESH,
            ).start()

        @pl.loop(0, CHUNK // 8)
        def _(half):
            to_partners(j * (CHUNK // 8) + half, ahead, give)

    def expert(x_in, gate, up, down, store):
        @pl.loop(0, gate.shape[1] // tile)
        def _(n):
            cols = pl.ds(pl.multiple_of(n * tile, tile), tile)
            hid_v[:, cols] = (silu(dot(x_in, gate[:, cols])) * dot(x_in, up[:, cols])).astype(BF16)

        hidden = hid_v[...]

        @pl.loop(0, width // tile)
        def _(n):
            cols = pl.ds(pl.multiple_of(n * tile, tile), tile)
            store(cols, dot(hidden, down[:, cols]))

    def keep_shared(cols, value):
        shared_v[:, cols] = ALPHA * normed_v[:, cols].astype(F32) + value

    loads[7].wait()
    loads[8].wait()
    loads[9].wait()
    expert(normed_v[...], sgate_v, sup_v, sdown_v, keep_shared)
    loads[10].wait()
    loads[11].wait()
    loads[12].wait()

    def waiter(ref, send, recv, j, first):
        part = ref.at[pl.ds(pl.multiple_of(j * CHUNK, CHUNK) + first, CHUNK - first)]
        return pltpu.make_async_remote_copy(
            src_ref=part, dst_ref=part, send_sem=send.at[j], recv_sem=recv.at[j],
            device_id={"sp": sp, "tp": 1 - tp}, device_id_type=MESH,
        )

    def serve(j, first):
        waiter(recv_v, go_send, go_recv, j, first).wait_recv()
        chosen = recv_v[pl.ds(j * CHUNK, CHUNK)]
        rows_v[...] = chosen.astype(F32).reshape(block, width).astype(BF16)

        def give(cols, value):
            res_v[pl.ds(j * CHUNK, CHUNK), :, cols] = value.reshape(CHUNK, slots, tile).astype(BF16)

        expert(rows_v[...], egate_v, eup_v, edown_v, give)

        def give_back(at, device):
            pltpu.make_async_remote_copy(
                src_ref=res_v.at[at], dst_ref=ret_v.at[at],
                send_sem=back_send.at[j], recv_sem=back_recv.at[j],
                device_id=device, device_id_type=MESH,
            ).start()

        @pl.loop(0, CHUNK // 8)
        def _(half):
            to_partners(j * (CHUNK // 8) + half, behind, give_back)

    recv_v[0] = send_v[0]
    serve(0, 1)
    ret_v[0] = res_v[0]

    @pl.loop(1, chunks)
    def _(j):
        serve(j, 0)

    def merge(q, first):
        waiter(ret_v, back_send, back_recv, 2 * q, first).wait_recv()
        waiter(ret_v, back_send, back_recv, 2 * q + 1, 0).wait_recv()
        share = merge_v[q]

        @pl.loop(0, width // tile)
        def _(n):
            cols = pl.ds(pl.multiple_of(n * tile, tile), tile)
            back = ret_v[pl.ds(2 * q * CHUNK, 2 * CHUNK), :, cols]
            back = back.astype(F32).reshape(2 * block, tile).astype(BF16)
            both = dot(share, back)
            shared_v[:, cols] += both[0:rows] + both[rows : 2 * rows]

    merge(0, 1)

    @pl.loop(1, chunks // 2)
    def _(q):
        merge(q, 0)

    @pl.loop(0, rows // 16, unroll=4)
    def _(b):
        at = pl.ds(pl.multiple_of(b * 16, 16), 16)
        out_ref[at, :] = layer_norm(shared_v[at, :], gout_ref[...]).astype(BF16)

    waiter(send_v, go_send, go_recv, 0, 1).wait_send()
    waiter(res_v, back_send, back_recv, 0, 1).wait_send()

    @pl.loop(1, chunks)
    def _(j):
        waiter(send_v, go_send, go_recv, j, 0).wait_send()
        waiter(res_v, back_send, back_recv, j, 0).wait_send()


def on_device(
    gate_pre, conv_in, conv_taps, recur_map, input_map, rate_logit, decay_shift, out_weight,
    residual, gain_mix, routes, route_weight, shared_gate, shared_up, shared_down,
    expert_gate, expert_up, expert_down, gain_out,
):
    tokens, channels = conv_in.shape
    rows, width = residual.shape
    heads, bw = recur_map.shape[:2]
    hidden = shared_gate.shape[1]
    groups, spans, peers, slots = channels // 128, tokens // SPAN, 2 * RING**3, 8
    any_spec = pl.BlockSpec(memory_space=pl.ANY)
    vmem_spec = pl.BlockSpec(memory_space=pltpu.VMEM)
    big = [
        gate_pre, conv_in, recur_map, input_map, out_weight, residual,
        shared_gate, shared_up, shared_down, expert_gate, expert_up, expert_down,
    ]
    small = [
        conv_taps, rate_logit.reshape(1, channels), decay_shift.T, gain_mix.reshape(1, width),
        gain_out.reshape(1, width), routes.T, route_weight.T,
    ]
    dma = pltpu.SemaphoreType.DMA
    chunks = peers // CHUNK
    return pl.pallas_call(
        layer_kernel,
        out_shape=jax.ShapeDtypeStruct((rows, width), BF16),
        in_specs=[any_spec] * (len(big) + len(small)),
        out_specs=vmem_spec,
        scratch_shapes=[pltpu.VMEM(v.shape, v.dtype) for v in small]
        + [
            pltpu.VMEM((tokens, 8), F32),
            pltpu.VMEM((tokens, channels), BF16),
            pltpu.VMEM((tokens, channels), BF16),
            pltpu.VMEM((heads, bw, bw), BF16),
            pltpu.VMEM((heads, bw, bw), BF16),
            pltpu.VMEM((2, channels, width), BF16),
            pltpu.VMEM((rows, width), BF16),
            pltpu.VMEM((width, hidden), BF16),
            pltpu.VMEM((width, hidden), BF16),
            pltpu.VMEM((hidden, width), BF16),
            pltpu.VMEM((width, hidden), BF16),
            pltpu.VMEM((width, hidden), BF16),
            pltpu.VMEM((hidden, width), BF16),
            pltpu.VMEM((HALO, channels), BF16),
            pltpu.VMEM((HALO + tokens, channels), F32),
            pltpu.VMEM((tokens, bw), F32),
            pltpu.VMEM((tokens, bw), F32),
            pltpu.VMEM((tokens, bw), BF16),
            pltpu.VMEM((groups, spans * PITCH, 128), F32),
            pltpu.VMEM((groups, spans * PITCH, 128), F32),
            pltpu.VMEM((groups, spans * PITCH, 128), F32),
            pltpu.VMEM((groups * spans, 128), F32),
            pltpu.VMEM((groups * spans, 128), F32),
            pltpu.VMEM((groups * spans, 128), F32),
            pltpu.VMEM((groups * spans, 128), F32),
            pltpu.VMEM((RING * RING, 2 * groups, 128), F32),
            pltpu.VMEM((RING, 2 * groups, 128), F32),
            pltpu.VMEM((tokens, channels), BF16),
            pltpu.VMEM((rows, channels), BF16),
            pltpu.VMEM((rows, width), F32),
            pltpu.VMEM((rows, width), BF16),
            pltpu.VMEM((rows, width), F32),
            pltpu.VMEM((CHUNK * slots, hidden), BF16),
            pltpu.VMEM((CHUNK * slots, width), BF16),
            pltpu.VMEM((peers * slots, rows), BF16),
            pltpu.VMEM((chunks // 2, 2 * rows, 2 * CHUNK * slots), BF16),
            pltpu.VMEM((peers, slots, width), BF16),
            pltpu.VMEM((peers, slots, width), BF16),
            pltpu.VMEM((peers, slots, width), BF16),
            pltpu.VMEM((peers, slots, width), BF16),
            dma((20,)), dma((2,)), dma((2,)), dma((2,)), dma((2,)),
            dma((chunks,)), dma((chunks,)), dma((chunks,)), dma((chunks,)),
        ],
        compiler_params=pltpu.CompilerParams(
            collective_id=0, has_side_effects=True, vmem_limit_bytes=52 * 1024 * 1024
        ),
        name="layer",
    )(*(pltpu.with_memory_space_constraint(v, pltpu.HBM) for v in (*big, *small)))


def solution(mesh):
    return jax.shard_map(
        on_device,
        mesh=mesh,
        in_specs=(
            P("sp", "tp"), P("sp", "tp"), P(None, "tp"), P("tp", None, None), P("tp", None, None),
            P("tp"), P("sp", "tp"), P(), P(("sp", "tp"), None), P(), P(("sp", "tp"), None),
            P(("sp", "tp"), None), P(), P(), P(), P(("sp", "tp"), None, None),
            P(("sp", "tp"), None, None), P(("sp", "tp"), None, None), P(),
        ),
        out_specs=P(("sp", "tp"), None),
        check_vma=False,
    )
```
